32 devices in a mesh: sp: 8 (over z, x), tp: 4 (over y, core).
Axes of the slice: x: 2, y: 2, z: 4, core: 2. Of those that a mesh axis runs over, the one named last changes fastest.
Arguments:
- residual: bfloat16 [1536, 2048], P('sp', 'tp'), may hold values from -10 to 10
- queries: bfloat16 [1536, 16, 128], P('sp', 'tp'), may hold values from -6.5 to 6.5
- key_rows: bfloat16 [1536, 16, 128], P('sp', 'tp'), may hold values from -6.5 to 6.5
- value_rows: bfloat16 [1536, 16, 128], P('sp', 'tp'), may hold values from -6 to 6
- diff_scale: float32 [16], P('tp'), may hold values from 0.3 to 0.8
- head_gain: float32 [128], replicated, may hold values from 0.1 to 1.9
- out_weight: bfloat16 [2048, 2048], P(None, 'tp'), may hold values from -0.125 to 0.125
- norm_gain: float32 [2048], replicated, may hold values from 0.1 to 1.9
- gate_weight: bfloat16 [8, 2048, 4096], P('sp', None, 'tp'), may hold values from -0.5 to 0.5
- up_weight: bfloat16 [8, 2048, 4096], P('sp', None, 'tp'), may hold values from -0.5 to 0.5
- down_weight: bfloat16 [8, 4096, 2048], P('sp', None, 'tp'), may hold values from -0.01171875 to 0.01171875
- expert_ids: int32 [1536, 2], P('sp'), may hold values from 0 to 7, all different within a row; in each aligned block of 192 rows (0 to 191, 192 to 383, ...) at most 96 rows name the same one
- route_logit: float32 [1536, 2], P('sp'), may hold values from -6 to 6
Outputs:
- updated: bfloat16 [1536, 2048], P('sp', 'tp')
The draws below stay inside these ranges and needn't reach their ends.
Inputs may be any that keep to these rules, and one draw needn't show every extreme that they name: `expert_ids`: A token's 2 experts differ. The 192 tokens of one index of sp name one expert at most 96 times, a bound that some block reaches on some index.
All inputs are finite; a program needn't handle non-finite values.
Results may differ from the reference program's by a relative error of at most 0.014.
Values may be sent and summed in bfloat16 or wider, within the bound.
A program may use at most 64 MiB of HBM per device.

```python
import math
import jax
import jax.numpy as jnp
import numpy as np
from jax import lax

D = 2048
HEADS = 16
QK = 64
V = 128
FF = 4096
TOP = 2
SPAN = 64
TOK_DEV = 192
TOKENS = 1536
EXPERTS = 8
CAP = 96
N_SP = 8


def drawn_pair(base):
    folded_key = jax.random.fold_in(base, 17)
    keys_list = jax.random.split(folded_key, 2)
    array_shape = (TOKENS, HEADS, 2 * QK)
    query_values = jnp.clip(1.3 * jax.random.normal(keys_list[0], array_shape, jnp.float32), -6.5, 6.5)
    key_values = jnp.clip(1.3 * jax.random.normal(keys_list[1], array_shape, jnp.float32), -6.5, 6.5)
    return (query_values, key_values)


def draw_queries(key, part):
    return drawn_pair(key)[0].astype(jnp.bfloat16)


def draw_key_rows(key, part):
    return drawn_pair(key)[1].astype(jnp.bfloat16)


def draw_residual(key, part):
    first = jax.random.fold_in(jax.random.fold_in(key, 29), 0)
    column = jnp.arange(D, dtype=jnp.float32) / D
    values = jnp.clip(jax.random.normal(first, (TOKENS, D), jnp.float32), -6.0, 6.0) * 0.5 * 3.0 ** column
    return values.astype(jnp.bfloat16)


def steps_of(rng, dims, cuts, least, top_value):
    factor_of, own = 1.0, jax.random.fold_in(rng, 6)
    for position, shards_of in cuts:
        steps = jnp.exp(jax.random.uniform(jax.random.fold_in(own, position), (shards_of,), jnp.float32, least / len(cuts), top_value / len(cuts)))
        factor_of = factor_of * jnp.repeat(steps, dims[position] // shards_of).reshape([-1 if axis == position else 1 for axis in range(len(dims))])
    return factor_of


def assign_block(rng, own, number, rows, number_of, top, limit, slope):
    sequence = jax.random.permutation(rng, number_of)
    packed, usual = portions_of(number_of, rows * top, limit, slope, True), portions_of(number_of, rows * top, limit, slope, False)
    places = jnp.arange(number_of)

    def named(tallies, offset_by):
        used = int((tallies > 0).sum())
        fixed = max(1, used // 4)
        passed = fixed + (places - fixed + offset_by * (used - fixed)) % max(1, number_of - fixed)
        return jnp.zeros((number_of,), jnp.int32).at[sequence[jnp.where(places < fixed, places, passed)]].set(jnp.asarray(tallies, jnp.int32))

    tallies = jnp.where(number % 4 == 0, named(packed, number // 4), named(usual, number - number // 4 - 1))
    mixed = jax.random.permutation(jax.random.fold_in(own, 3), number_of)
    donor, taker = mixed[0:number_of // 2 * 2:2], mixed[1:number_of // 2 * 2:2]
    margin = jnp.minimum(tallies[donor] - 1, limit - tallies[taker]) // 2
    margin = jnp.where((donor == sequence[0]) | (taker == sequence[0]) | (tallies[taker] == 0), 0, jnp.maximum(margin, 0))
    passed = jax.random.randint(jax.random.fold_in(own, 4), (number_of // 2,), 0, 1 << 20) % (margin + 1)
    tallies = tallies.at[donor].add(-passed).at[taker].add(passed)
    items = jnp.searchsorted(jnp.cumsum(tallies), jnp.arange(rows * top), side="right").astype(jnp.int32)
    listing = items.reshape(top, rows).T
    listing = listing[jax.random.permutation(jax.random.fold_in(own, 1), rows)]
    offset_by = jax.random.randint(jax.random.fold_in(own, 2), (rows, 1), 0, top)
    return jnp.take_along_axis(listing, (jnp.arange(top)[None, :] + offset_by) % top, axis=1)


def portions_of(number_of, total, reach, skew, full):
    portions = [(1 << 20) // math.isqrt(grade ** skew) + 1 for grade in range(1, number_of + 1)]
    largest = reach if full else min(reach, max(-(-total // number_of), total * portions[0] // sum(portions)))
    least = 1 if total - largest >= number_of - 1 else 0
    counts, rest = [largest] + [least] * (number_of - 1), total - largest - least * (number_of - 1)
    while rest > 0:
        free = [i for i in range(1, number_of) if counts[i] < largest] or [i for i in range(1, number_of) if counts[i] < reach]
        pool, remaining = sum([portions[i] for i in free]), rest
        for i in free:
            more = min(reach - counts[i], max(1, remaining * portions[i] // pool), rest)
            counts[i] = counts[i] + more
            rest = rest - more
    return np.array(counts)


def centred(own_key, extent, deviation, most, pieces=(), held_as=jnp.bfloat16):
    values = deviation * jax.random.normal(own_key, extent, jnp.float32)
    if pieces:
        values = values * steps_of(own_key, extent, pieces, -0.22, 0.18)
    return jnp.clip(values, -most, most).astype(held_as)


def setup_inputs(seed: int = 0) -> dict:
    keys = jax.random.split(jax.random.key(seed), 14)
    residual = draw_residual(jax.random.fold_in(keys[13], 71), 0)
    queries = draw_queries(jax.random.fold_in(keys[13], 71), 0)
    key_rows = draw_key_rows(jax.random.fold_in(keys[13], 71), 0)
    value_rows = centred(keys[3], (TOKENS, HEADS, V), 1.0, 6.0, ((0, 8), (1, 4)))
    diff_scale = jnp.clip(0.3 + 0.5 * jax.random.uniform(keys[4], (HEADS,), jnp.float32) ** steps_of(keys[4], (HEADS,), ((0, 4),), -0.2, 0.2), 0.3, 0.8)
    head_gain = jnp.clip(1.0 + 0.18 * jax.random.normal(keys[5], (V,), jnp.float32), 0.1, 1.9)
    out_weight = centred(keys[6], (HEADS * V, D), (HEADS * V) ** -0.5, 0.125, ((1, 4),))
    norm_gain = jnp.clip(1.0 + 0.18 * jax.random.normal(keys[7], (D,), jnp.float32), 0.1, 1.9)
    gate_weight = centred(keys[8], (EXPERTS, D, FF), (D // 16) ** -0.5, 0.5, ((0, 8), (2, 4)))
    up_weight = centred(keys[9], (EXPERTS, D, FF), (D // 16) ** -0.5, 0.5, ((0, 8), (2, 4)))
    down_weight = centred(keys[10], (EXPERTS, FF, D), (FF * 64) ** -0.5, 0.01171875, ((0, 8), (2, 4)))
    expert_ids_keys = jax.random.split(jax.random.fold_in(keys[11], 1), TOKENS // TOK_DEV)
    expert_ids_turns = jax.random.permutation(jax.random.fold_in(keys[11], 3), TOKENS // TOK_DEV)
    expert_ids = jax.vmap(lambda own, number: assign_block(jax.random.fold_in(keys[11], 2), own, number, TOK_DEV, EXPERTS, TOP, CAP, 2))(expert_ids_keys, expert_ids_turns).reshape((TOKENS, TOP))
    route_logit = centred(keys[12], (TOKENS, TOP), 1.5, 6.0, ((0, 8),), jnp.float32)
    return {"residual": residual, "queries": queries, "key_rows": key_rows, "value_rows": value_rows, "diff_scale": diff_scale, "head_gain": head_gain, "out_weight": out_weight, "norm_gain": norm_gain, "gate_weight": gate_weight, "up_weight": up_weight, "down_weight": down_weight, "expert_ids": expert_ids, "route_logit": route_logit}


NORM_EPS = 1e-05
CLAMP_LIMIT = 7.0
SWISH_ALPHA = 1.702
HEAD_KEEP = 0.8

def one_map(query_half, key_half, value_all, visible):
    scores = jnp.einsum('qhd,khd->hqk', query_half, key_half) * QK ** (-0.5)
    scores = jnp.where(visible[None], scores, -jnp.inf)
    row_peak = lax.optimization_barrier(jnp.max(scores, axis=-1, keepdims=True))
    exp_weights = jnp.where(visible[None], jnp.exp(scores - row_peak), 0.0)
    row_total = lax.optimization_barrier(jnp.sum(exp_weights, axis=-1))
    rounded = lax.optimization_barrier(exp_weights.astype(jnp.bfloat16)).astype(jnp.float32)
    accum = jnp.einsum('hqk,khv->hqv', rounded, value_all)
    return accum / row_total[..., None]

def reference(residual, queries, key_rows, value_rows, diff_scale, head_gain, out_weight, norm_gain, gate_weight, up_weight, down_weight, expert_ids, route_logit):
    block_rows = math.gcd(TOKENS, 512)
    key_all = key_rows.astype(jnp.float32)
    value_all = value_rows.astype(jnp.float32)
    key_span = jnp.arange(TOKENS, dtype=jnp.int32) // SPAN

    def attend(block_index):
        first_row = (block_index * block_rows).astype(jnp.int32)
        query_block = lax.dynamic_slice_in_dim(queries, first_row, block_rows, 0).astype(jnp.float32)
        query_span = (first_row + jnp.arange(block_rows, dtype=jnp.int32)) // SPAN
        visible = key_span[None, :] <= query_span[:, None]
        first_map = one_map(query_block[..., :QK], key_all[..., :QK], value_all, visible)
        second_map = one_map(query_block[..., QK:], key_all[..., QK:], value_all, visible)
        mixture = first_map - diff_scale[:, None, None] * second_map
        scale_back = lax.rsqrt(lax.optimization_barrier(jnp.mean(mixture * mixture, axis=-1, keepdims=True)) + NORM_EPS)
        attended = (mixture * scale_back * head_gain * HEAD_KEEP).astype(jnp.bfloat16)
        return jnp.transpose(attended, (1, 0, 2)).reshape(block_rows, HEADS * V)
    attended = lax.map(attend, jnp.arange(TOKENS // block_rows, dtype=jnp.int32)).reshape(TOKENS, HEADS * V)
    projected = jnp.dot(attended, out_weight, preferred_element_type=jnp.float32)
    after_mixer = (residual.astype(jnp.float32) + projected).astype(jnp.bfloat16)
    mixer_float = after_mixer.astype(jnp.float32)
    square_total = lax.optimization_barrier(jnp.sum(mixer_float * mixer_float, axis=-1, keepdims=True))
    normed = (mixer_float * lax.rsqrt(square_total / D + NORM_EPS) * norm_gain).astype(jnp.bfloat16)
    chosen = expert_ids.reshape(N_SP, TOK_DEV * TOP)
    onehot = (chosen[..., None] == jnp.arange(EXPERTS, dtype=jnp.int32)).astype(jnp.int32)
    rank_in = (lax.optimization_barrier(jnp.sum(jnp.cumsum(onehot, axis=1).astype(jnp.int32) * onehot, axis=-1)) - 1).astype(jnp.int32)
    source = jnp.arange(N_SP, dtype=jnp.int32)[:, None]
    per_expert = N_SP * CAP
    slot_index = (chosen * per_expert + source * CAP + rank_in).reshape(TOKENS * TOP).astype(jnp.int32)
    token_of = jnp.arange(TOKENS * TOP, dtype=jnp.int32) // TOP
    owner_row = jnp.full((EXPERTS * per_expert,), TOKENS, jnp.int32).at[slot_index].set(token_of)
    padded = jnp.concatenate([normed, jnp.zeros((1, D), jnp.bfloat16)], axis=0)

    def run_expert(expert):
        rows_in = padded[lax.dynamic_slice_in_dim(owner_row, (expert * per_expert).astype(jnp.int32), per_expert, 0)]
        pre_gate = jnp.dot(rows_in, gate_weight[expert], preferred_element_type=jnp.float32)
        pre_up = jnp.dot(rows_in, up_weight[expert], preferred_element_type=jnp.float32)
        capped = jnp.minimum(pre_gate, CLAMP_LIMIT)
        linear = jnp.clip(pre_up, -CLAMP_LIMIT, CLAMP_LIMIT)
        hidden = (capped * jax.nn.sigmoid(SWISH_ALPHA * capped) * (linear + 1.0)).astype(jnp.bfloat16)
        return jnp.dot(hidden, down_weight[expert], preferred_element_type=jnp.float32).astype(jnp.bfloat16)
    expert_out = lax.map(run_expert, jnp.arange(EXPERTS, dtype=jnp.int32)).reshape(EXPERTS * per_expert, D)
    picked = expert_out[slot_index].astype(jnp.float32).reshape(TOKENS, TOP, D)
    weights = jax.nn.softmax(route_logit.astype(jnp.float32), axis=-1)
    routed = lax.optimization_barrier(jnp.sum(picked * weights[..., None], axis=1))
    return (mixer_float + routed).astype(jnp.bfloat16)
```

```python
import functools
import math

import jax
import jax.numpy as jnp
from jax import lax
from jax.experimental import pallas as pl
from jax.experimental.pallas import tpu as pltpu
from jax.sharding import PartitionSpec as P

D = 2048
QK = 64
SPAN = 64


NORM_EPS = 1e-05
CLAMP_LIMIT = 7.0
SWISH_ALPHA = 1.702
HEAD_KEEP = 0.8
NEG_FILL = -1e30
MESH = pl.DeviceIdType.MESH
F32 = jnp.float32
BF16 = jnp.bfloat16


def layer_kernel(
    sp_size,
    tp_size,
    groups,
    cap,
    early,
    residual,
    queries,
    own_block,
    diff_scale,
    head_gain,
    out_hbm,
    norm_gain,
    gate_hbm,
    up_hbm,
    down_hbm,
    expert_ids,
    route_logit,
    updated,
    scaled,
    blocks,
    peak,
    total,
    accum,
    heads_all,
    out_w,
    mixer,
    places,
    outgoing,
    rows_in,
    normed,
    hidden,
    down_part,
    own_sum,
    part_send,
    part_recv,
    result,
    returned,
    gate,
    up,
    weight_sem,
    block_sem,
    along_send,
    across_send,
    kv_recv,
    down_send,
    down_recv,
    att_send,
    att_recv,
    disp_send,
    disp_recv,
    row_send,
    row_recv,
    hid_send,
    hid_recv,
    sum_send,
    sum_recv,
    ret_send,
    ret_recv,
):
    me = lax.axis_index("sp")
    rank = lax.axis_index("tp")
    parity = lax.rem(rank, 2)
    sibling = rank + 1 - 2 * parity
    chips = tp_size // 2
    chip = rank // 2
    span = sp_size // groups
    rows = span * cap
    tokens = queries.shape[0]
    width = head_gain.shape[1]
    heads = queries.shape[1] // width
    feats = residual.shape[1]
    units = gate.shape[1]
    columns = feats
    tops = expert_ids.shape[1]

    def at(index):
        return {"sp": index, "tp": rank}

    def beside(target):
        return {"sp": me, "tp": target}

    def peer_rank(step):
        return lax.rem(chip + step, chips) * 2 + parity

    def remote(src, dst, send, recv, device):
        return pltpu.make_async_remote_copy(
            src_ref=src,
            dst_ref=dst,
            send_sem=send,
            recv_sem=recv,
            device_id=device,
            device_id_type=MESH,
        )

    load = pltpu.make_async_copy(own_block, blocks.at[me], block_sem)
    load.start()
    pieces = down_send.shape[1]
    chunk = 2 * units // pieces
    weights = [
        pltpu.make_async_copy(out_hbm, out_w, weight_sem.at[0]),
        pltpu.make_async_copy(gate_hbm, gate, weight_sem.at[1]),
        pltpu.make_async_copy(up_hbm, up, weight_sem.at[2]),
        pltpu.make_async_copy(
            down_hbm.at[pl.ds(chip * 2 * units, 2 * units)], down_part.at[chip], weight_sem.at[3]
        ),
    ]
    for copy in weights:
        copy.start()

    barrier = pltpu.get_barrier_semaphore()
    for step in range(1, sp_size):
        pl.semaphore_signal(
            barrier, inc=1, device_id=at(lax.rem(me + step, sp_size)), device_id_type=MESH
        )
    for step in range(1, chips):
        pl.semaphore_signal(barrier, inc=1, device_id=beside(peer_rank(step)), device_id_type=MESH)
    pl.semaphore_signal(barrier, inc=1, device_id=beside(sibling), device_id_type=MESH)

    scaled[...] = (queries[...].astype(F32) * QK ** (-0.5)).astype(BF16)
    total[...] = jnp.zeros(total.shape, F32)
    accum[...] = jnp.zeros(accum.shape, F32)
    peak[...] = jnp.full(peak.shape, NEG_FILL, F32)

    lane = lax.broadcasted_iota(jnp.int32, (tokens, 128), 1)
    named = [lane == expert_ids[:, k : k + 1] for k in range(tops)]
    both = functools.reduce(jnp.logical_or, named).astype(F32).astype(BF16)
    before = (
        lax.broadcasted_iota(jnp.int32, (tokens, tokens), 1)
        < lax.broadcasted_iota(jnp.int32, (tokens, tokens), 0)
    ).astype(F32).astype(BF16)
    earlier = jnp.dot(before, both, preferred_element_type=F32)
    for k in range(tops):
        order = jnp.sum(jnp.where(named[k], earlier, 0.0), axis=1, keepdims=True)
        step_of = lax.rem(me + sp_size - expert_ids[:, k : k + 1], sp_size)
        places[:, k : k + 1] = step_of * cap + order.astype(jnp.int32)

    pl.semaphore_wait(barrier, sp_size - 1 + chips)

    def down_piece(step, piece):
        target = lax.rem(chip + step, chips)
        return remote(
            down_hbm.at[pl.ds(target * 2 * units + piece * chunk, chunk)],
            down_part.at[chip, pl.ds(piece * chunk, chunk)],
            down_send.at[step - 1, piece],
            down_recv.at[chip, piece],
            beside(target * 2 + parity),
        )

    def send_down(first, last):
        for step in range(1, chips):
            @pl.loop(first, last)
            def _(piece):
                down_piece(step, piece).start()

    load.wait()

    pairs = sp_size // 2
    pair = me // 2
    side = lax.rem(me, 2)
    other = me + 1 - 2 * side

    def hand_on(block, send, back, target):
        return remote(
            blocks.at[block], blocks.at[block], send.at[back], kv_recv.at[block], at(target)
        )

    def attend(block, masked):
        if masked:
            row = me * tokens + lax.broadcasted_iota(jnp.int32, (tokens, tokens), 0)
            col = block * tokens + lax.broadcasted_iota(jnp.int32, (tokens, tokens), 1)
            visible = col // SPAN <= row // SPAN
        for head in range(heads):
            value = blocks[block, 1, :, head * width : (head + 1) * width]
            for half in range(2):
                start = head * width + half * QK
                scores = lax.dot_general(
                    scaled[:, start : start + QK],
                    blocks[block, 0, :, start : start + QK],
                    (((1,), (1,)), ((), ())),
                    preferred_element_type=F32,
                )
                if masked:
                    scores = jnp.where(visible, scores, NEG_FILL)
                index = head * 2 + half
                old = peak[index]
                new = jnp.maximum(old, jnp.max(scores, axis=-1, keepdims=True))
                exps = jnp.exp(scores - new)
                if masked:
                    exps = jnp.where(visible, exps, 0.0)
                rescale = jnp.exp(old - new)
                peak[index] = new
                total[index] = total[index] * rescale + jnp.sum(exps, axis=-1, keepdims=True)
                accum[index] = accum[index] * rescale + jnp.dot(
                    exps.astype(BF16), value, preferred_element_type=F32
                )

    plain_blocks = tokens % SPAN == 0

    @pl.loop(0, pair + 2)
    def _(back):
        @pl.when(back <= pair)
        def _():
            block = me - 2 * back

            @pl.when(back > 0)
            def _():
                hand_on(block, across_send, back, other).wait_recv()

            @pl.when(pair < pairs - 1)
            def _():
                hand_on(block, along_send, back, me + 2).start()

            @pl.when((back > 0) | (side == 0))
            def _():
                hand_on(block, across_send, back, other).start()

        @pl.when(back == 0)
        def _():
            send_down(0, early)
            attend(me, True)

        second = other - 2 * (back - 1)
        use_second = (back >= 2) | ((back == 1) & (side == 1))

        @pl.loop(0, 2)
        def _(which):
            @pl.when((which == 1) & use_second)
            def _():
                hand_on(second, across_send, 0, other).wait_recv()

            @pl.when(((which == 0) & (back > 0) & (back <= pair)) | ((which == 1) & use_second))
            def _():
                attend(jnp.where(which == 0, me - 2 * back, second), not plain_blocks)

    def piece(buffer, send, recv, owner, target, send_slot):
        return remote(
            buffer.at[owner],
            buffer.at[owner],
            send.at[send_slot],
            recv.at[owner],
            beside(target),
        )

    def spread(buffer, send, recv):
        for step in range(1, chips):
            target = peer_rank(step)
            piece(buffer, send, recv, rank, target, target).start()
        piece(buffer, send, recv, rank, sibling, sibling).start()

    def forward(buffer, send, recv, step):
        owner = peer_rank(step)
        onward = piece(buffer, send, recv, owner, sibling, owner + 1 - 2 * parity)
        onward.wait_recv()
        onward.start()

    def collect(buffer, send, recv):
        for step in range(1, chips):
            forward(buffer, send, recv, step)
        for step in range(chips):
            owner = peer_rank(step) + 1 - 2 * parity
            piece(buffer, send, recv, owner, sibling, sibling).wait_recv()

    def settle(buffer, send, recv):
        for step in range(1, chips):
            target = peer_rank(step)
            piece(buffer, send, recv, rank, target, target).wait_send()
            piece(buffer, send, recv, target, sibling, target + 1 - 2 * parity).wait_send()
        piece(buffer, send, recv, rank, sibling, sibling).wait_send()

    for head in range(heads):
        first = accum[head * 2] / total[head * 2]
        later = accum[head * 2 + 1] / total[head * 2 + 1]
        mixture = first - diff_scale[head] * later
        scale_back = lax.rsqrt(jnp.mean(mixture * mixture, axis=-1, keepdims=True) + NORM_EPS)
        heads_all[rank, :, head * width : (head + 1) * width] = (
            mixture * scale_back * head_gain[...] * HEAD_KEEP
        ).astype(BF16)
    spread(heads_all, att_send, att_recv)
    send_down(early, pieces)
    weights[0].wait()

    def project(owner):
        return jnp.dot(
            heads_all[owner],
            out_w[pl.ds(pl.multiple_of(owner * heads * width, heads * width), heads * width)],
            preferred_element_type=F32,
        )

    sums = own_sum.at[0, pl.ds(0, tokens)]
    sums[...] = residual[...].astype(F32) + project(rank)
    collect(heads_all, att_send, att_recv)
    for step in range(chips):
        owner = peer_rank(step) + 1 - 2 * parity
        sums[...] += project(owner)
        if step > 0:
            sums[...] += project(peer_rank(step))
    mixer[...] = sums[...].astype(BF16)

    def slots_of(first, count):
        slot = first + lax.broadcasted_iota(jnp.int32, (tokens, count), 1)
        return [
            (slot == places[:, k : k + 1]).astype(F32).astype(BF16) for k in range(tops)
        ]

    def chosen_rows(step):
        held = functools.reduce(jnp.add, slots_of(step * cap, cap))
        return lax.dot_general(
            held, mixer[...], (((0,), (0,)), ((), ())), preferred_element_type=F32
        ).astype(BF16)

    def dispatch(step):
        expert = lax.rem(me + sp_size - step, sp_size)
        return remote(
            outgoing.at[step],
            rows_in.at[step // span, rank, pl.ds(lax.rem(step, span) * cap, cap)],
            disp_send.at[step],
            disp_recv.at[step],
            at(expert),
        )

    rows_in[0, rank, pl.ds(0, cap), :] = chosen_rows(0)

    @pl.loop(1, sp_size)
    def _(step):
        outgoing[step] = chosen_rows(step)
        dispatch(step).start()

    unit_tile = math.gcd(units, 256)
    column_tile = math.gcd(columns, 256)

    def spread_rows(group):
        for place in range(span):
            step = group * span + place
            arrived = remote(
                outgoing.at[0],
                rows_in.at[group, rank, pl.ds(place * cap, cap)],
                disp_send.at[step],
                disp_recv.at[step],
                beside(sibling),
            )
            if place == 0:
                @pl.when(group > 0)
                def _():
                    arrived.wait_recv()
            else:
                arrived.wait_recv()
        spread(rows_in.at[group], row_send.at[group], row_recv.at[group])

    def hidden_copy(group):
        return remote(
            hidden.at[group, parity],
            hidden.at[group, parity],
            hid_send.at[group],
            hid_recv.at[group],
            beside(sibling),
        )

    def run_up(group):
        collect(rows_in.at[group], row_send.at[group], row_recv.at[group])

        @pl.when(group == 0)
        def _():
            weights[1].wait()
            weights[2].wait()

        square = 0.0
        for part in range(tp_size):
            value = rows_in[group, part].astype(F32)
            square += jnp.sum(value * value, axis=-1, keepdims=True)
        scale_back = lax.rsqrt(square / (tp_size * feats) + NORM_EPS)
        for part in range(tp_size):
            depth = slice(part * feats, (part + 1) * feats)
            normed[:, depth] = (
                rows_in[group, part].astype(F32) * scale_back * norm_gain[:, depth]
            ).astype(BF16)

        @pl.loop(0, units // unit_tile)
        def _(tile):
            cols = pl.ds(pl.multiple_of(tile * unit_tile, unit_tile), unit_tile)
            pre_gate = jnp.dot(normed[...], gate[:, cols], preferred_element_type=F32)
            pre_up = jnp.dot(normed[...], up[:, cols], preferred_element_type=F32)
            capped = jnp.minimum(pre_gate, CLAMP_LIMIT)
            linear = jnp.clip(pre_up, -CLAMP_LIMIT, CLAMP_LIMIT)
            value = capped * jax.nn.sigmoid(SWISH_ALPHA * capped) * (linear + 1.0)
            hidden[group, parity, :, cols] = value.astype(BF16)

        hidden_copy(group).start()

    def sum_copy(group, step):
        target = lax.rem(chip + step, chips)
        return remote(
            part_send.at[group, step - 1],
            part_recv.at[group, step - 1],
            sum_send.at[group, step - 1],
            sum_recv.at[group, step - 1],
            beside(target * 2 + parity),
        )

    def part_sum(group, block, cols):
        value = 0.0
        for core in range(2):
            value += jnp.dot(
                hidden[group, core],
                down_part[block, core * units : (core + 1) * units, cols],
                preferred_element_type=F32,
            )
        return value

    def run_down(group):
        remote(
            hidden.at[group, 1 - parity],
            hidden.at[group, 1 - parity],
            hid_send.at[group],
            hid_recv.at[group],
            beside(sibling),
        ).wait_recv()

        @pl.when(group == 0)
        def _():
            weights[3].wait()
            for step in range(1, chips):
                source = lax.rem(chip + step, chips)

                @pl.loop(0, pieces)
                def _(index):
                    remote(
                        down_part.at[source, pl.ds(index * chunk, chunk)],
                        down_part.at[source, pl.ds(index * chunk, chunk)],
                        down_send.at[step - 1, index],
                        down_recv.at[source, index],
                        beside(sibling),
                    ).wait_recv()

        for step in range(1, chips):
            @pl.loop(0, columns // column_tile)
            def _(tile):
                cols = pl.ds(pl.multiple_of(tile * column_tile, column_tile), column_tile)
                part_send[group, step - 1, :, cols] = part_sum(
                    group, lax.rem(chip + step, chips), cols
                ).astype(BF16)

            sum_copy(group, step).start()

        @pl.loop(0, columns // column_tile)
        def _(tile):
            cols = pl.ds(pl.multiple_of(tile * column_tile, column_tile), column_tile)
            own_sum[lax.rem(group, 2), pl.ds(0, rows), cols] = part_sum(group, chip, cols)

    def give_back(group, place):
        step = group * span + place
        return remote(
            result.at[group, pl.ds(place * cap, cap)],
            returned.at[group, pl.ds(place * cap, cap)],
            ret_send.at[step],
            ret_recv.at[step],
            at(lax.rem(me + step, sp_size)),
        )

    def finish(group):
        value = own_sum[lax.rem(group, 2), pl.ds(0, rows), :]
        for step in range(1, chips):
            sum_copy(group, step).wait_recv()
            value += part_recv[group, step - 1].astype(F32)
        result[group] = value.astype(BF16)
        for place in range(span):
            if place == 0:
                @pl.when(group == 0)
                def _():
                    returned[0, pl.ds(0, cap), :] = result[0, pl.ds(0, cap), :]

                @pl.when(group > 0)
                def _():
                    give_back(group, 0).start()
            else:
                give_back(group, place).start()

    @pl.loop(0, groups + 3)
    def _(turn):
        @pl.when(turn < groups)
        def _():
            spread_rows(turn)

        @pl.when((turn >= 1) & (turn < groups + 1))
        def _():
            run_up(turn - 1)

        @pl.when((turn >= 3))
        def _():
            finish(turn - 3)

        @pl.when((turn >= 2) & (turn < groups + 2))
        def _():
            run_down(turn - 2)

    peak_logit = jnp.max(route_logit[...], axis=-1, keepdims=True)
    shares = jnp.exp(route_logit[...] - peak_logit)
    shares = shares / jnp.sum(shares, axis=-1, keepdims=True)
    back_sum = own_sum.at[0, pl.ds(0, tokens)]
    back_sum[...] = mixer[...].astype(F32)

    @pl.loop(0, groups)
    def _(group):
        for place in range(span):
            if place == 0:
                @pl.when(group > 0)
                def _():
                    give_back(group, 0).wait_recv()
            else:
                give_back(group, place).wait_recv()
        routed = 0.0
        for k, held in enumerate(slots_of(group * rows, rows)):
            picked = jnp.dot(held, returned[group], preferred_element_type=F32)
            routed += picked * shares[:, k : k + 1]
        back_sum[...] += routed

    updated[...] = back_sum[...].astype(BF16)

    @pl.loop(0, pair + 1)
    def _(back):
        block = me - 2 * back

        @pl.when(pair < pairs - 1)
        def _():
            hand_on(block, along_send, back, me + 2).wait_send()

        @pl.when((back > 0) | (side == 0))
        def _():
            hand_on(block, across_send, back, other).wait_send()

    for step in range(1, chips):
        @pl.loop(0, pieces)
        def _(index):
            down_piece(step, index).wait_send()

    settle(heads_all, att_send, att_recv)

    @pl.loop(1, sp_size)
    def _(step):
        dispatch(step).wait_send()

    @pl.loop(0, groups)
    def _(group):
        settle(rows_in.at[group], row_send.at[group], row_recv.at[group])
        hidden_copy(group).wait_send()
        for step in range(1, chips):
            sum_copy(group, step).wait_send()
        for place in range(span):
            if place == 0:
                @pl.when(group > 0)
                def _():
                    give_back(group, 0).wait_send()
            else:
                give_back(group, place).wait_send()


def local(
    residual,
    queries,
    key_rows,
    value_rows,
    diff_scale,
    head_gain,
    out_weight,
    norm_gain,
    gate_weight,
    up_weight,
    down_weight,
    expert_ids,
    route_logit,
):
    sp_size = lax.axis_size("sp")
    tp_size = lax.axis_size("tp")
    tokens, heads, width = value_rows.shape
    feats = residual.shape[1]
    flat = heads * width
    own_block = jnp.stack([key_rows.reshape(tokens, flat), value_rows.reshape(tokens, flat)])
    tops = expert_ids.shape[1]
    cap = -(-(2 * tokens * tops // sp_size) // 16) * 16
    groups = math.gcd(sp_size, 4)
    span = sp_size // groups
    rows = span * cap
    units = gate_weight.shape[2]
    chips = tp_size // 2
    pieces = 8
    early = 6
    dma = pltpu.SemaphoreType.DMA
    vmem = pl.BlockSpec(memory_space=pltpu.VMEM)
    hbm = pl.BlockSpec(memory_space=pl.ANY)
    return pl.pallas_call(
        functools.partial(layer_kernel, sp_size, tp_size, groups, cap, early),
        out_shape=jax.ShapeDtypeStruct((tokens, feats), BF16),
        in_specs=[
            vmem,
            vmem,
            hbm,
            pl.BlockSpec(memory_space=pltpu.SMEM),
            vmem,
            hbm,
            vmem,
            hbm,
            hbm,
            hbm,
            vmem,
            vmem,
        ],
        out_specs=vmem,
        scratch_shapes=[
            pltpu.VMEM((tokens, flat), BF16),
            pltpu.VMEM((sp_size,) + own_block.shape, BF16),
            pltpu.VMEM((heads * 2, tokens, 1), F32),
            pltpu.VMEM((heads * 2, tokens, 1), F32),
            pltpu.VMEM((heads * 2, tokens, width), F32),
            pltpu.VMEM((tp_size, tokens, flat), BF16),
            pltpu.VMEM(out_weight.shape, BF16),
            pltpu.VMEM((tokens, feats), BF16),
            pltpu.VMEM((tokens, tops), jnp.int32),
            pltpu.VMEM((sp_size, cap, feats), BF16),
            pltpu.VMEM((groups, tp_size, rows, feats), BF16),
            pltpu.VMEM((rows, tp_size * feats), BF16),
            pltpu.VMEM((groups, 2, rows, units), BF16),
            pltpu.VMEM((chips, 2 * units, feats), BF16),
            pltpu.VMEM((2, max(rows, tokens), feats), F32),
            pltpu.VMEM((groups, max(chips - 1, 1), rows, feats), BF16),
            pltpu.VMEM((groups, max(chips - 1, 1), rows, feats), BF16),
            pltpu.VMEM((groups, rows, feats), BF16),
            pltpu.VMEM((groups, rows, feats), BF16),
            pltpu.VMEM(gate_weight.shape[1:], BF16),
            pltpu.VMEM(up_weight.shape[1:], BF16),
            dma((4,)),
            dma(()),
            dma((sp_size,)),
            dma((sp_size,)),
            dma((sp_size,)),
            dma((max(chips - 1, 1), pieces)),
            dma((chips, pieces)),
            dma((tp_size,)),
            dma((tp_size,)),
            dma((sp_size,)),
            dma((sp_size,)),
            dma((groups, tp_size)),
            dma((groups, tp_size)),
            dma((groups,)),
            dma((groups,)),
            dma((groups, max(chips - 1, 1))),
            dma((groups, max(chips - 1, 1))),
            dma((sp_size,)),
            dma((sp_size,)),
        ],
        compiler_params=pltpu.CompilerParams(
            collective_id=0, has_side_effects=True, vmem_limit_bytes=56 * 1024 * 1024
        ),
    )(
        residual,
        queries.reshape(tokens, flat),
        own_block,
        diff_scale,
        head_gain[None],
        out_weight,
        norm_gain[None],
        gate_weight[0],
        up_weight[0],
        down_weight[0],
        expert_ids,
        route_logit,
    )


def solution(mesh):
    return jax.shard_map(
        local,
        mesh=mesh,
        in_specs=(
            P("sp", "tp"),
            P("sp", "tp", None),
            P("sp", "tp", None),
            P("sp", "tp", None),
            P("tp"),
            P(),
            P(None, "tp"),
            P(),
            P("sp", None, "tp"),
            P("sp", None, "tp"),
            P("sp", None, "tp"),
            P("sp", None),
            P("sp", None),
        ),
        out_specs=P("sp", "tp"),
        check_vma=False,
    )
```

```python
import functools
import math

import jax
import jax.numpy as jnp
from jax import lax
from jax.experimental import pallas as pl
from jax.experimental.pallas import tpu as pltpu
from jax.sharding import PartitionSpec as P

D = 2048
QK = 64
SPAN = 64


NORM_EPS = 1e-05
CLAMP_LIMIT = 7.0
SWISH_ALPHA = 1.702
HEAD_KEEP = 0.8
NEG_FILL = -1e30
MESH = pl.DeviceIdType.MESH
F32 = jnp.float32
BF16 = jnp.bfloat16


def layer_kernel(
    sp_size,
    tp_size,
    groups,
    cap,
    early,
    residual_hbm,
    query_hbm,
    key_hbm,
    value_hbm,
    diff_scale,
    head_gain,
    out_hbm,
    norm_gain,
    gate_hbm,
    up_hbm,
    down_hbm,
    expert_ids,
    route_logit,
    updated,
    residual,
    raw,
    scaled,
    blocks,
    peak,
    accum,
    heads_all,
    out_w,
    mixer,
    places,
    outgoing,
    rows_in,
    normed,
    hidden,
    down_part,
    own_sum,
    part_send,
    part_recv,
    result,
    returned,
    gate,
    up,
    weight_sem,
    raw_sem,
    along_send,
    across_send,
    kv_recv,
    down_send,
    down_recv,
    att_send,
    att_recv,
    disp_send,
    disp_recv,
    row_send,
    row_recv,
    hid_send,
    hid_recv,
    sum_send,
    sum_recv,
    ret_send,
    ret_recv,
):
    me = lax.axis_index("sp")
    rank = lax.axis_index("tp")
    parity = lax.rem(rank, 2)
    sibling = rank + 1 - 2 * parity
    chips = tp_size // 2
    chip = rank // 2
    span = sp_size // groups
    rows = span * cap
    tokens, heads, width = query_hbm.shape
    feats = residual.shape[1]
    units = gate.shape[1]
    columns = feats
    tops = expert_ids.shape[0]

    def at(index):
        return {"sp": index, "tp": rank}

    def beside(target):
        return {"sp": me, "tp": target}

    def peer_rank(step):
        return lax.rem(chip + step, chips) * 2 + parity

    def remote(src, dst, send, recv, device):
        return pltpu.make_async_remote_copy(
            src_ref=src,
            dst_ref=dst,
            send_sem=send,
            recv_sem=recv,
            device_id=device,
            device_id_type=MESH,
        )

    raw_loads = [
        pltpu.make_async_copy(source, raw.at[i], raw_sem.at[i])
        for i, source in enumerate((key_hbm, value_hbm, query_hbm))
    ]
    for copy in raw_loads:
        copy.start()
    pieces = down_send.shape[1]
    chunk = 2 * units // pieces
    weights = [
        pltpu.make_async_copy(out_hbm, out_w, weight_sem.at[0]),
        pltpu.make_async_copy(gate_hbm, gate, weight_sem.at[1]),
        pltpu.make_async_copy(up_hbm, up, weight_sem.at[2]),
        pltpu.make_async_copy(
            down_hbm.at[pl.ds(chip * 2 * units, 2 * units)], down_part.at[chip], weight_sem.at[3]
        ),
        pltpu.make_async_copy(residual_hbm, residual, weight_sem.at[4]),
    ]

    barrier = pltpu.get_barrier_semaphore()
    for step in range(1, sp_size):
        pl.semaphore_signal(
            barrier, inc=1, device_id=at(lax.rem(me + step, sp_size)), device_id_type=MESH
        )
    for step in range(1, chips):
        pl.semaphore_signal(barrier, inc=1, device_id=beside(peer_rank(step)), device_id_type=MESH)
    pl.semaphore_signal(barrier, inc=1, device_id=beside(sibling), device_id_type=MESH)

    accum[...] = jnp.zeros(accum.shape, F32)
    peak[...] = jnp.full(peak.shape, NEG_FILL, F32)

    spare = -(-sp_size // 16) * 16
    names = lax.broadcasted_iota(jnp.int32, (spare, tokens), 0)
    named = [names == expert_ids[k : k + 1] for k in range(tops)]
    both = functools.reduce(jnp.logical_or, named).astype(F32).astype(BF16)
    before = (
        lax.broadcasted_iota(jnp.int32, (tokens, tokens), 0)
        < lax.broadcasted_iota(jnp.int32, (tokens, tokens), 1)
    ).astype(F32).astype(BF16)
    earlier = jnp.dot(both, before, preferred_element_type=F32)
    peak_logit = jnp.max(route_logit[...], axis=0, keepdims=True)
    shares = jnp.exp(route_logit[...] - peak_logit)
    shares = shares / jnp.sum(shares, axis=0, keepdims=True)
    for k in range(tops):
        order = jnp.sum(jnp.where(named[k], earlier, 0.0), axis=0, keepdims=True)
        step_of = lax.rem(me + sp_size - expert_ids[k : k + 1], sp_size)
        places[k : k + 1] = step_of * cap + order.astype(jnp.int32)

    for i in range(2):
        raw_loads[i].wait()
        blocks[me, i] = jnp.transpose(raw[i], (1, 0, 2))
    raw_loads[2].wait()
    low = lax.broadcasted_iota(jnp.int32, (heads, tokens, width), 2) < QK
    query = jnp.transpose(raw[2], (1, 0, 2)).astype(F32) * QK ** (-0.5)
    scaled[0] = jnp.where(low, query, 0.0).astype(BF16)
    scaled[1] = jnp.where(low, 0.0, query).astype(BF16)

    pl.semaphore_wait(barrier, sp_size - 1 + chips)

    def down_piece(step, piece):
        target = lax.rem(chip + step, chips)
        return remote(
            down_hbm.at[pl.ds(target * 2 * units + piece * chunk, chunk)],
            down_part.at[chip, pl.ds(piece * chunk, chunk)],
            down_send.at[step - 1, piece],
            down_recv.at[chip, piece],
            beside(target * 2 + parity),
        )

    def send_down(first, last):
        for step in range(1, chips):
            @pl.loop(first, last)
            def _(piece):
                down_piece(step, piece).start()

    pairs = sp_size // 2
    pair = me // 2
    side = lax.rem(me, 2)
    other = me + 1 - 2 * side

    def hand_on(block, send, back, target):
        return remote(
            blocks.at[block], blocks.at[block], send.at[back], kv_recv.at[block], at(target)
        )

    def attend(block, masked):
        if masked:
            key = block * tokens + lax.broadcasted_iota(jnp.int32, (tokens, tokens), 0)
            query = me * tokens + lax.broadcasted_iota(jnp.int32, (tokens, tokens), 1)
            visible = key // SPAN <= query // SPAN
        for head in range(heads):
            value = jnp.concatenate(
                [jnp.transpose(blocks[block, 1, head]), jnp.ones((16, tokens), BF16)], axis=0
            )
            for half in range(2):
                scores = lax.dot_general(
                    blocks[block, 0, head],
                    scaled[half, head],
                    (((1,), (1,)), ((), ())),
                    preferred_element_type=F32,
                )
                if masked:
                    scores = jnp.where(visible, scores, NEG_FILL)
                index = head * 2 + half
                old = peak[index]
                new = jnp.maximum(old, jnp.max(scores, axis=0, keepdims=True))
                exps = jnp.exp(scores - new)
                if masked:
                    exps = jnp.where(visible, exps, 0.0)
                peak[index] = new
                accum[index] = accum[index] * jnp.exp(old - new) + jnp.dot(
                    value, exps.astype(BF16), preferred_element_type=F32
                )

    plain_blocks = tokens % SPAN == 0

    @pl.loop(0, pair + 2)
    def _(back):
        @pl.when(back <= pair)
        def _():
            block = me - 2 * back

            @pl.when(back > 0)
            def _():
                hand_on(block, across_send, back, other).wait_recv()

            @pl.when(pair < pairs - 1)
            def _():
                hand_on(block, along_send, back, me + 2).start()

            @pl.when((back > 0) | (side == 0))
            def _():
                hand_on(block, across_send, back, other).start()

        @pl.when(back == 0)
        def _():
            send_down(0, early)
            for copy in weights:
                copy.start()
            attend(me, True)

        second = other - 2 * (back - 1)
        use_second = (back >= 2) | ((back == 1) & (side == 1))

        @pl.loop(0, 2)
        def _(which):
            @pl.when((which == 1) & use_second)
            def _():
                hand_on(second, across_send, 0, other).wait_recv()

            @pl.when(((which == 0) & (back > 0) & (back <= pair)) | ((which == 1) & use_second))
            def _():
                attend(jnp.where(which == 0, me - 2 * back, second), not plain_blocks)

    def piece(buffer, send, recv, owner, target, send_slot):
        return remote(
            buffer.at[owner],
            buffer.at[owner],
            send.at[send_slot],
            recv.at[owner],
            beside(target),
        )

    def spread(buffer, send, recv):
        for step in range(1, chips):
            target = peer_rank(step)
            piece(buffer, send, recv, rank, target, target).start()
        piece(buffer, send, recv, rank, sibling, sibling).start()

    def forward(buffer, send, recv, step):
        owner = peer_rank(step)
        onward = piece(buffer, send, recv, owner, sibling, owner + 1 - 2 * parity)
        onward.wait_recv()
        onward.start()

    def collect(buffer, send, recv):
        for step in range(1, chips):
            forward(buffer, send, recv, step)
        for step in range(chips):
            owner = peer_rank(step) + 1 - 2 * parity
            piece(buffer, send, recv, owner, sibling, sibling).wait_recv()

    def settle(buffer, send, recv):
        for step in range(1, chips):
            target = peer_rank(step)
            piece(buffer, send, recv, rank, target, target).wait_send()
            piece(buffer, send, recv, target, sibling, target + 1 - 2 * parity).wait_send()
        piece(buffer, send, recv, rank, sibling, sibling).wait_send()

    for head in range(heads):
        maps = [
            accum[index, :width] / accum[index, width : width + 1]
            for index in (head * 2, head * 2 + 1)
        ]
        mixture = maps[0] - diff_scale[head] * maps[1]
        scale_back = lax.rsqrt(jnp.mean(mixture * mixture, axis=0, keepdims=True) + NORM_EPS)
        heads_all[head, rank] = (
            jnp.transpose(mixture * scale_back) * head_gain[...] * HEAD_KEEP
        ).astype(BF16)
        spread(heads_all.at[head], att_send.at[head], att_recv.at[head])
    send_down(early, pieces)
    weights[0].wait()
    weights[4].wait()

    def project(owner):
        return jnp.dot(
            jnp.concatenate([heads_all[head, owner] for head in range(heads)], axis=1),
            out_w[pl.ds(pl.multiple_of(owner * heads * width, heads * width), heads * width)],
            preferred_element_type=F32,
        )

    sums = own_sum.at[0, pl.ds(0, tokens)]
    sums[...] = residual[...].astype(F32) + project(rank)
    for head in range(heads):
        for step in range(1, chips):
            forward(heads_all.at[head], att_send.at[head], att_recv.at[head], step)

    def from_sibling(step):
        owner = peer_rank(step) + 1 - 2 * parity
        for head in range(heads):
            piece(
                heads_all.at[head], att_send.at[head], att_recv.at[head], owner, sibling, sibling
            ).wait_recv()
        return project(owner)

    sums[...] += from_sibling(0)
    for step in range(1, chips):
        sums[...] += project(peer_rank(step))
    for step in range(1, chips):
        sums[...] += from_sibling(step)
    mixer[...] = sums[...].astype(BF16)

    def slots_of(first, count):
        slot = first + lax.broadcasted_iota(jnp.int32, (count, tokens), 0)
        return [slot == places[k : k + 1] for k in range(tops)]

    def chosen_rows(step):
        held = functools.reduce(jnp.logical_or, slots_of(step * cap, cap))
        return jnp.dot(
            held.astype(F32).astype(BF16), mixer[...], preferred_element_type=F32
        ).astype(BF16)

    def dispatch(step):
        expert = lax.rem(me + sp_size - step, sp_size)
        return remote(
            outgoing.at[step],
            rows_in.at[step // span, rank, pl.ds(lax.rem(step, span) * cap, cap)],
            disp_send.at[step],
            disp_recv.at[step],
            at(expert),
        )

    rows_in[0, rank, pl.ds(0, cap), :] = chosen_rows(0)

    @pl.loop(1, sp_size)
    def _(step):
        outgoing[step] = chosen_rows(step)
        dispatch(step).start()

    unit_tile = math.gcd(units, 256)
    column_tile = math.gcd(columns, 256)

    def spread_rows(group):
        for place in range(span):
            step = group * span + place
            arrived = remote(
                outgoing.at[0],
                rows_in.at[group, rank, pl.ds(place * cap, cap)],
                disp_send.at[step],
                disp_recv.at[step],
                beside(sibling),
            )
            if place == 0:
                @pl.when(group > 0)
                def _():
                    arrived.wait_recv()
            else:
                arrived.wait_recv()
        spread(rows_in.at[group], row_send.at[group], row_recv.at[group])

    def hidden_copy(group):
        return remote(
            hidden.at[group, parity],
            hidden.at[group, parity],
            hid_send.at[group],
            hid_recv.at[group],
            beside(sibling),
        )

    def run_up(group):
        collect(rows_in.at[group], row_send.at[group], row_recv.at[group])

        @pl.when(group == 0)
        def _():
            weights[1].wait()
            weights[2].wait()

        square = 0.0
        for part in range(tp_size):
            value = rows_in[group, part].astype(F32)
            square += jnp.sum(value * value, axis=-1, keepdims=True)
        scale_back = lax.rsqrt(square / (tp_size * feats) + NORM_EPS)
        for part in range(tp_size):
            depth = slice(part * feats, (part + 1) * feats)
            normed[:, depth] = (
                rows_in[group, part].astype(F32) * scale_back * norm_gain[:, depth]
            ).astype(BF16)

        @pl.loop(0, units // unit_tile)
        def _(tile):
            cols = pl.ds(pl.multiple_of(tile * unit_tile, unit_tile), unit_tile)
            pre_gate = jnp.dot(normed[...], gate[:, cols], preferred_element_type=F32)
            pre_up = jnp.dot(normed[...], up[:, cols], preferred_element_type=F32)
            capped = jnp.minimum(pre_gate, CLAMP_LIMIT)
            linear = jnp.clip(pre_up, -CLAMP_LIMIT, CLAMP_LIMIT)
            value = capped * jax.nn.sigmoid(SWISH_ALPHA * capped) * (linear + 1.0)
            hidden[group, parity, :, cols] = value.astype(BF16)

        hidden_copy(group).start()

    def sum_copy(group, step):
        target = lax.rem(chip + step, chips)
        return remote(
            part_send.at[group, step - 1],
            part_recv.at[group, step - 1],
            sum_send.at[group, step - 1],
            sum_recv.at[group, step - 1],
            beside(target * 2 + parity),
        )

    def part_sum(group, block, cols):
        value = 0.0
        for core in range(2):
            value += jnp.dot(
                hidden[group, core],
                down_part[block, core * units : (core + 1) * units, cols],
                preferred_element_type=F32,
            )
        return value

    def run_down(group):
        remote(
            hidden.at[group, 1 - parity],
            hidden.at[group, 1 - parity],
            hid_send.at[group],
            hid_recv.at[group],
            beside(sibling),
        ).wait_recv()

        @pl.when(group == 0)
        def _():
            weights[3].wait()
            for step in range(1, chips):
                source = lax.rem(chip + step, chips)

                @pl.loop(0, pieces)
                def _(index):
                    remote(
                        down_part.at[source, pl.ds(index * chunk, chunk)],
                        down_part.at[source, pl.ds(index * chunk, chunk)],
                        down_send.at[step - 1, index],
                        down_recv.at[source, index],
                        beside(sibling),
                    ).wait_recv()

        for step in range(1, chips):
            @pl.loop(0, columns // column_tile)
            def _(tile):
                cols = pl.ds(pl.multiple_of(tile * column_tile, column_tile), column_tile)
                part_send[group, step - 1, :, cols] = part_sum(
                    group, lax.rem(chip + step, chips), cols
                ).astype(BF16)

            sum_copy(group, step).start()

        @pl.loop(0, columns // column_tile)
        def _(tile):
            cols = pl.ds(pl.multiple_of(tile * column_tile, column_tile), column_tile)
            own_sum[lax.rem(group, 2), pl.ds(0, rows), cols] = part_sum(group, chip, cols)

    def give_back(group, place):
        step = group * span + place
        return remote(
            result.at[group, pl.ds(place * cap, cap)],
            returned.at[group, pl.ds(place * cap, cap)],
            ret_send.at[step],
            ret_recv.at[step],
            at(lax.rem(me + step, sp_size)),
        )

    def finish(group):
        value = own_sum[lax.rem(group, 2), pl.ds(0, rows), :]
        for step in range(1, chips):
            sum_copy(group, step).wait_recv()
            value += part_recv[group, step - 1].astype(F32)
        result[group] = value.astype(BF16)
        for place in range(span):
            if place == 0:
                @pl.when(group == 0)
                def _():
                    returned[0, pl.ds(0, cap), :] = result[0, pl.ds(0, cap), :]

                @pl.when(group > 0)
                def _():
                    give_back(group, 0).start()
            else:
                give_back(group, place).start()

    @pl.loop(0, groups + 3)
    def _(turn):
        @pl.when(turn < groups)
        def _():
            spread_rows(turn)

        @pl.when((turn >= 1) & (turn < groups + 1))
        def _():
            run_up(turn - 1)

        @pl.when((turn >= 3))
        def _():
            finish(turn - 3)

        @pl.when((turn >= 2) & (turn < groups + 2))
        def _():
            run_down(turn - 2)

    back_sum = own_sum.at[0, pl.ds(0, tokens)]
    back_sum[...] = mixer[...].astype(F32)

    @pl.loop(0, groups)
    def _(group):
        for place in range(span):
            if place == 0:
                @pl.when(group > 0)
                def _():
                    give_back(group, 0).wait_recv()
            else:
                give_back(group, place).wait_recv()
        portion = 0.0
        for k, held in enumerate(slots_of(group * rows, rows)):
            portion += jnp.where(held, shares[k : k + 1], 0.0)
        coarse = portion.astype(BF16)
        fine = (portion - coarse.astype(F32)).astype(BF16)
        routed = 0.0
        for part in (coarse, fine):
            routed += lax.dot_general(
                part, returned[group], (((0,), (0,)), ((), ())), preferred_element_type=F32
            )
        back_sum[...] += routed

    updated[...] = back_sum[...].astype(BF16)

    @pl.loop(0, pair + 1)
    def _(back):
        block = me - 2 * back

        @pl.when(pair < pairs - 1)
        def _():
            hand_on(block, along_send, back, me + 2).wait_send()

        @pl.when((back > 0) | (side == 0))
        def _():
            hand_on(block, across_send, back, other).wait_send()

    for step in range(1, chips):
        @pl.loop(0, pieces)
        def _(index):
            down_piece(step, index).wait_send()

    for head in range(heads):
        settle(heads_all.at[head], att_send.at[head], att_recv.at[head])

    @pl.loop(1, sp_size)
    def _(step):
        dispatch(step).wait_send()

    @pl.loop(0, groups)
    def _(group):
        settle(rows_in.at[group], row_send.at[group], row_recv.at[group])
        hidden_copy(group).wait_send()
        for step in range(1, chips):
            sum_copy(group, step).wait_send()
        for place in range(span):
            if place == 0:
                @pl.when(group > 0)
                def _():
                    give_back(group, 0).wait_send()
            else:
                give_back(group, place).wait_send()


def local(
    residual,
    queries,
    key_rows,
    value_rows,
    diff_scale,
    head_gain,
    out_weight,
    norm_gain,
    gate_weight,
    up_weight,
    down_weight,
    expert_ids,
    route_logit,
):
    sp_size = lax.axis_size("sp")
    tp_size = lax.axis_size("tp")
    tokens, heads, width = value_rows.shape
    feats = residual.shape[1]
    tops = expert_ids.shape[1]
    cap = -(-(2 * tokens * tops // sp_size) // 16) * 16
    groups = math.gcd(sp_size, 4)
    span = sp_size // groups
    rows = span * cap
    units = gate_weight.shape[2]
    chips = tp_size // 2
    pieces = 16
    early = 13
    dma = pltpu.SemaphoreType.DMA
    vmem = pl.BlockSpec(memory_space=pltpu.VMEM)
    hbm = pl.BlockSpec(memory_space=pl.ANY)
    return pl.pallas_call(
        functools.partial(layer_kernel, sp_size, tp_size, groups, cap, early),
        out_shape=jax.ShapeDtypeStruct((tokens, feats), BF16),
        in_specs=[
            hbm,
            hbm,
            hbm,
            hbm,
            pl.BlockSpec(memory_space=pltpu.SMEM),
            vmem,
            hbm,
            vmem,
            hbm,
            hbm,
            hbm,
            vmem,
            vmem,
        ],
        out_specs=vmem,
        scratch_shapes=[
            pltpu.VMEM((tokens, feats), BF16),
            pltpu.VMEM((3, tokens, heads, width), BF16),
            pltpu.VMEM((2, heads, tokens, width), BF16),
            pltpu.VMEM((sp_size, 2, heads, tokens, width), BF16),
            pltpu.VMEM((heads * 2, 1, tokens), F32),
            pltpu.VMEM((heads * 2, width + 16, tokens), F32),
            pltpu.VMEM((heads, tp_size, tokens, width), BF16),
            pltpu.VMEM(out_weight.shape, BF16),
            pltpu.VMEM((tokens, feats), BF16),
            pltpu.VMEM((tops, tokens), jnp.int32),
            pltpu.VMEM((sp_size, cap, feats), BF16),
            pltpu.VMEM((groups, tp_size, rows, feats), BF16),
            pltpu.VMEM((rows, tp_size * feats), BF16),
            pltpu.VMEM((groups, 2, rows, units), BF16),
            pltpu.VMEM((chips, 2 * units, feats), BF16),
            pltpu.VMEM((2, max(rows, tokens), feats), F32),
            pltpu.VMEM((groups, max(chips - 1, 1), rows, feats), BF16),
            pltpu.VMEM((groups, max(chips - 1, 1), rows, feats), BF16),
            pltpu.VMEM((groups, rows, feats), BF16),
            pltpu.VMEM((groups, rows, feats), BF16),
            pltpu.VMEM(gate_weight.shape[1:], BF16),
            pltpu.VMEM(up_weight.shape[1:], BF16),
            dma((5,)),
            dma((3,)),
            dma((sp_size,)),
            dma((sp_size,)),
            dma((sp_size,)),
            dma((max(chips - 1, 1), pieces)),
            dma((chips, pieces)),
            dma((heads, tp_size)),
            dma((heads, tp_size)),
            dma((sp_size,)),
            dma((sp_size,)),
            dma((groups, tp_size)),
            dma((groups, tp_size)),
            dma((groups,)),
            dma((groups,)),
            dma((groups, max(chips - 1, 1))),
            dma((groups, max(chips - 1, 1))),
            dma((sp_size,)),
            dma((sp_size,)),
        ],
        compiler_params=pltpu.CompilerParams(
            collective_id=0, has_side_effects=True, vmem_limit_bytes=56 * 1024 * 1024
        ),
    )(
        residual,
        queries,
        key_rows,
        value_rows,
        diff_scale,
        head_gain[None],
        out_weight,
        norm_gain[None],
        gate_weight[0],
        up_weight[0],
        down_weight[0],
        expert_ids.T,
        route_logit.T,
    )


def solution(mesh):
    return jax.shard_map(
        local,
        mesh=mesh,
        in_specs=(
            P("sp", "tp"),
            P("sp", "tp", None),
            P("sp", "tp", None),
            P("sp", "tp", None),
            P("tp"),
            P(),
            P(None, "tp"),
            P(),
            P("sp", None, "tp"),
            P("sp", None, "tp"),
            P("sp", None, "tp"),
            P("sp", None),
            P("sp", None),
        ),
        out_specs=P("sp", "tp"),
        check_vma=False,
    )
```

```python
import functools
import math

import jax
import jax.numpy as jnp
from jax import lax
from jax.experimental import pallas as pl
from jax.experimental.pallas import tpu as pltpu
from jax.sharding import PartitionSpec as P

D = 2048
QK = 64
SPAN = 64


NORM_EPS = 1e-05
CLAMP_LIMIT = 7.0
SWISH_ALPHA = 1.702
HEAD_KEEP = 0.8
NEG_FILL = -1e30
MESH = pl.DeviceIdType.MESH
F32 = jnp.float32
BF16 = jnp.bfloat16


def layer_kernel(
    sp_size,
    tp_size,
    groups,
    cap,
    early,
    residual_hbm,
    query_hbm,
    key_hbm,
    value_hbm,
    diff_scale,
    head_gain,
    out_hbm,
    norm_gain,
    gate_hbm,
    up_hbm,
    down_hbm,
    expert_ids,
    route_logit,
    updated,
    residual,
    raw,
    scaled,
    blocks,
    peak,
    accum,
    heads_all,
    out_w,
    mixer,
    places,
    near_out,
    far_out,
    near_rows,
    far_rows,
    normed,
    near_hidden,
    far_hidden,
    down_part,
    own_sum,
    far_sum,
    part_send,
    part_recv,
    near_result,
    far_result,
    near_back,
    far_back,
    share_send,
    share_recv,
    gate,
    up,
    weight_sem,
    raw_sem,
    along_send,
    across_send,
    kv_recv,
    down_send,
    down_recv,
    att_send,
    att_recv,
    mix_send,
    mix_recv,
    near_send,
    near_recv,
    far_send,
    far_recv,
    pair_send,
    pair_recv,
    row_send,
    row_recv,
    hid_send,
    hid_recv,
    sum_send,
    sum_recv,
    near_ret_send,
    near_ret_recv,
    far_ret_send,
    far_ret_recv,
    share_send_sem,
    share_recv_sem,
):
    me = lax.axis_index("sp")
    rank = lax.axis_index("tp")
    parity = lax.rem(rank, 2)
    sibling = rank + 1 - 2 * parity
    chips = tp_size // 2
    chip = rank // 2
    reach = sp_size // 2
    half_of = me // reach
    spot = lax.rem(me, reach)
    span = reach // groups
    rows = span * cap
    near_count = reach * cap
    tokens, heads, width = query_hbm.shape
    feats = residual.shape[1]
    units = gate.shape[1]
    columns = feats
    tops = expert_ids.shape[0]

    def at(index):
        return {"sp": index, "tp": rank}

    def beside(target):
        return {"sp": me, "tp": target}

    def peer_rank(step):
        return lax.rem(chip + step, chips) * 2 + parity

    def remote(src, dst, send, recv, device):
        return pltpu.make_async_remote_copy(
            src_ref=src,
            dst_ref=dst,
            send_sem=send,
            recv_sem=recv,
            device_id=device,
            device_id_type=MESH,
        )

    raw_loads = [
        pltpu.make_async_copy(source, raw.at[i], raw_sem.at[i])
        for i, source in enumerate((key_hbm, value_hbm, query_hbm))
    ]
    for copy in raw_loads:
        copy.start()
    pieces = down_send.shape[1]
    chunk = 2 * units // pieces
    weights = [
        pltpu.make_async_copy(out_hbm, out_w, weight_sem.at[0]),
        pltpu.make_async_copy(gate_hbm, gate, weight_sem.at[1]),
        pltpu.make_async_copy(up_hbm, up, weight_sem.at[2]),
        pltpu.make_async_copy(
            down_hbm.at[pl.ds(chip * 2 * units, 2 * units)], down_part.at[chip], weight_sem.at[3]
        ),
        pltpu.make_async_copy(residual_hbm, residual, weight_sem.at[4]),
    ]

    barrier = pltpu.get_barrier_semaphore()
    for step in range(1, sp_size):
        pl.semaphore_signal(
            barrier, inc=1, device_id=at(lax.rem(me + step, sp_size)), device_id_type=MESH
        )
    for step in range(1, chips):
        pl.semaphore_signal(barrier, inc=1, device_id=beside(peer_rank(step)), device_id_type=MESH)
    pl.semaphore_signal(barrier, inc=1, device_id=beside(sibling), device_id_type=MESH)

    accum[...] = jnp.zeros(accum.shape, F32)
    peak[...] = jnp.full(peak.shape, NEG_FILL, F32)

    spare = -(-sp_size // 16) * 16
    names = lax.broadcasted_iota(jnp.int32, (spare, tokens), 0)
    named = [names == expert_ids[k : k + 1] for k in range(tops)]
    both = functools.reduce(jnp.logical_or, named).astype(F32).astype(BF16)
    before = (
        lax.broadcasted_iota(jnp.int32, (tokens, tokens), 0)
        < lax.broadcasted_iota(jnp.int32, (tokens, tokens), 1)
    ).astype(F32).astype(BF16)
    earlier = jnp.dot(both, before, preferred_element_type=F32)
    peak_logit = jnp.max(route_logit[...], axis=0, keepdims=True)
    shares = jnp.exp(route_logit[...] - peak_logit)
    shares = shares / jnp.sum(shares, axis=0, keepdims=True)
    for k in range(tops):
        order = jnp.sum(jnp.where(named[k], earlier, 0.0), axis=0, keepdims=True)
        expert = expert_ids[k : k + 1]
        apart = jnp.where(expert // reach == half_of, 0, reach)
        step_of = lax.rem(spot + reach - lax.rem(expert, reach), reach) + apart
        places[k : k + 1] = step_of * cap + order.astype(jnp.int32)

    for i in range(2):
        raw_loads[i].wait()
        blocks[me, i] = jnp.transpose(raw[i], (1, 0, 2))
    raw_loads[2].wait()
    low = lax.broadcasted_iota(jnp.int32, (heads, tokens, width), 2) < QK
    query = jnp.transpose(raw[2], (1, 0, 2)).astype(F32) * QK ** (-0.5)
    scaled[0] = jnp.where(low, query, 0.0).astype(BF16)
    scaled[1] = jnp.where(low, 0.0, query).astype(BF16)

    pl.semaphore_wait(barrier, sp_size - 1 + chips)

    def down_piece(step, piece):
        target = lax.rem(chip + step, chips)
        return remote(
            down_hbm.at[pl.ds(target * 2 * units + piece * chunk, chunk)],
            down_part.at[chip, pl.ds(piece * chunk, chunk)],
            down_send.at[step - 1, piece],
            down_recv.at[chip, piece],
            beside(target * 2 + parity),
        )

    def send_down(first, last):
        for step in range(1, chips):
            @pl.loop(first, last)
            def _(piece):
                down_piece(step, piece).start()

    pairs = sp_size // 2
    pair = me // 2
    side = lax.rem(me, 2)
    other = me + 1 - 2 * side

    def hand_on(block, send, back, target):
        return remote(
            blocks.at[block], blocks.at[block], send.at[back], kv_recv.at[block], at(target)
        )

    def attend(block, masked):
        if masked:
            key = block * tokens + lax.broadcasted_iota(jnp.int32, (tokens, tokens), 0)
            query = me * tokens + lax.broadcasted_iota(jnp.int32, (tokens, tokens), 1)
            visible = key // SPAN <= query // SPAN
        for head in range(heads):
            value = jnp.concatenate(
                [jnp.transpose(blocks[block, 1, head]), jnp.ones((16, tokens), BF16)], axis=0
            )
            for half in range(2):
                scores = lax.dot_general(
                    blocks[block, 0, head],
                    scaled[half, head],
                    (((1,), (1,)), ((), ())),
                    preferred_element_type=F32,
                )
                if masked:
                    scores = jnp.where(visible, scores, NEG_FILL)
                index = head * 2 + half
                old = peak[index]
                new = jnp.maximum(old, jnp.max(scores, axis=0, keepdims=True))
                exps = jnp.exp(scores - new)
                if masked:
                    exps = jnp.where(visible, exps, 0.0)
                peak[index] = new
                accum[index] = accum[index] * jnp.exp(old - new) + jnp.dot(
                    value, exps.astype(BF16), preferred_element_type=F32
                )

    plain_blocks = tokens % SPAN == 0

    @pl.loop(0, pair + 2)
    def _(back):
        @pl.when(back <= pair)
        def _():
            block = me - 2 * back

            @pl.when(back > 0)
            def _():
                hand_on(block, across_send, back, other).wait_recv()

            @pl.when(pair < pairs - 1)
            def _():
                hand_on(block, along_send, back, me + 2).start()

            @pl.when((back > 0) | (side == 0))
            def _():
                hand_on(block, across_send, back, other).start()

        @pl.when(back == 0)
        def _():
            send_down(0, early)
            for copy in weights:
                copy.start()
            attend(me, True)

        second = other - 2 * (back - 1)
        use_second = (back >= 2) | ((back == 1) & (side == 1))

        @pl.loop(0, 2)
        def _(which):
            @pl.when((which == 1) & use_second)
            def _():
                hand_on(second, across_send, 0, other).wait_recv()

            @pl.when(((which == 0) & (back > 0) & (back <= pair)) | ((which == 1) & use_second))
            def _():
                attend(jnp.where(which == 0, me - 2 * back, second), not plain_blocks)

    def piece(buffer, send, recv, owner, target, send_slot):
        return remote(
            buffer.at[owner],
            buffer.at[owner],
            send.at[send_slot],
            recv.at[owner],
            beside(target),
        )

    def spread(buffer, send, recv):
        for step in range(1, chips):
            target = peer_rank(step)
            piece(buffer, send, recv, rank, target, target).start()
        piece(buffer, send, recv, rank, sibling, sibling).start()

    def forward(buffer, send, recv, step):
        owner = peer_rank(step)
        onward = piece(buffer, send, recv, owner, sibling, owner + 1 - 2 * parity)
        onward.wait_recv()
        onward.start()

    def collect(buffer, send, recv):
        for step in range(1, chips):
            forward(buffer, send, recv, step)
        for step in range(chips):
            owner = peer_rank(step) + 1 - 2 * parity
            piece(buffer, send, recv, owner, sibling, sibling).wait_recv()

    def settle(buffer, send, recv):
        for step in range(1, chips):
            target = peer_rank(step)
            piece(buffer, send, recv, rank, target, target).wait_send()
            piece(buffer, send, recv, target, sibling, target + 1 - 2 * parity).wait_send()
        piece(buffer, send, recv, rank, sibling, sibling).wait_send()

    for head in range(heads):
        maps = [
            accum[index, :width] / accum[index, width : width + 1]
            for index in (head * 2, head * 2 + 1)
        ]
        mixture = maps[0] - diff_scale[head] * maps[1]
        scale_back = lax.rsqrt(jnp.mean(mixture * mixture, axis=0, keepdims=True) + NORM_EPS)
        heads_all[head, rank] = (
            jnp.transpose(mixture * scale_back) * head_gain[...] * HEAD_KEEP
        ).astype(BF16)
        spread(heads_all.at[head], att_send.at[head], att_recv.at[head])
    send_down(early, pieces)
    weights[0].wait()
    weights[4].wait()

    def project(owner):
        return jnp.dot(
            jnp.concatenate([heads_all[head, owner] for head in range(heads)], axis=1),
            out_w[pl.ds(pl.multiple_of(owner * heads * width, heads * width), heads * width)],
            preferred_element_type=F32,
        )

    sums = own_sum
    sums[...] = residual[...].astype(F32) + project(rank)
    for head in range(heads):
        for step in range(1, chips):
            forward(heads_all.at[head], att_send.at[head], att_recv.at[head], step)

    def from_sibling(step):
        owner = peer_rank(step) + 1 - 2 * parity
        for head in range(heads):
            piece(
                heads_all.at[head], att_send.at[head], att_recv.at[head], owner, sibling, sibling
            ).wait_recv()
        return project(owner)

    sums[...] += from_sibling(0)
    for step in range(1, chips):
        sums[...] += project(peer_rank(step))
    for step in range(1, chips):
        sums[...] += from_sibling(step)
    mixer[chip] = sums[...].astype(BF16)

    def mix_copy(step):
        target = lax.rem(chip + step, chips)
        return remote(
            mixer.at[chip],
            mixer.at[chip],
            mix_send.at[step - 1],
            mix_recv.at[chip],
            beside(target * 2 + parity),
        )

    for step in range(1, chips):
        mix_copy(step).start()

    def slots_of(first, count):
        slot = first + lax.broadcasted_iota(jnp.int32, (count, tokens), 0)
        return [slot == places[k : k + 1] for k in range(tops)]

    def chosen_rows(step, source):
        held = functools.reduce(jnp.logical_or, slots_of(step * cap, cap))
        return jnp.dot(
            held.astype(F32).astype(BF16), mixer[source], preferred_element_type=F32
        ).astype(BF16)

    def near_at(place):
        return at(half_of * reach + lax.rem(spot + reach + place, reach))

    def far_at(place):
        return at((1 - half_of) * reach + lax.rem(spot + reach + place, reach))

    def far_dispatch(place):
        return remote(
            far_out.at[place],
            far_rows.at[place // span, rank, pl.ds(lax.rem(place, span) * cap, cap)],
            far_send.at[place],
            far_recv.at[place],
            far_at(-place),
        )

    def near_dispatch(place, source):
        return remote(
            near_out.at[place, source],
            near_rows.at[source * 2 + parity, pl.ds(place * cap, cap)],
            near_send.at[place, source],
            near_recv.at[place, source],
            near_at(-place),
        )

    def send_near(source):
        near_rows[source * 2 + parity, pl.ds(0, cap), :] = chosen_rows(0, source)

        @pl.loop(1, reach)
        def _(place):
            near_out[place, source] = chosen_rows(place, source)
            near_dispatch(place, source).start()

    @pl.loop(0, reach)
    def _(place):
        far_out[place] = chosen_rows(reach + place, chip)
        far_dispatch(place).start()

    send_near(chip)
    for step in range(1, chips):
        source = lax.rem(chip + step, chips)
        remote(
            mixer.at[source],
            mixer.at[source],
            mix_send.at[step - 1],
            mix_recv.at[source],
            beside(sibling),
        ).wait_recv()
        send_near(source)

    unit_tile = math.gcd(units, 256)
    column_tile = math.gcd(columns, 256)

    def spread_rows(group):
        for place in range(span):
            remote(
                far_out.at[0],
                far_rows.at[group, rank, pl.ds(place * cap, cap)],
                far_send.at[group * span + place],
                far_recv.at[group * span + place],
                beside(sibling),
            ).wait_recv()
        spread(far_rows.at[group], row_send.at[group], row_recv.at[group])

    def pair_copy(source):
        return remote(
            near_rows.at[source * 2 + parity],
            near_rows.at[source * 2 + parity],
            pair_send.at[source],
            pair_recv.at[source],
            beside(sibling),
        )

    def pair_rows():
        for step in range(chips):
            source = lax.rem(chip + step, chips)

            @pl.loop(1, reach)
            def _(place):
                remote(
                    near_out.at[0, 0],
                    near_rows.at[source * 2 + parity, pl.ds(place * cap, cap)],
                    near_send.at[place, source],
                    near_recv.at[place, source],
                    beside(sibling),
                ).wait_recv()

            pair_copy(source).start()

    def pair_wait():
        for step in range(chips):
            source = lax.rem(chip + step, chips)
            remote(
                near_rows.at[source * 2 + 1 - parity],
                near_rows.at[source * 2 + 1 - parity],
                pair_send.at[source],
                pair_recv.at[source],
                beside(sibling),
            ).wait_recv()

    def hidden_copy(hidden, index, core):
        return remote(
            hidden.at[core],
            hidden.at[core],
            hid_send.at[index],
            hid_recv.at[index],
            beside(sibling),
        )

    def run_up(table, hidden, count, index):
        square = 0.0
        for part in range(tp_size):
            value = table[part].astype(F32)
            square += jnp.sum(value * value, axis=-1, keepdims=True)
        scale_back = lax.rsqrt(square / (tp_size * feats) + NORM_EPS)
        for part in range(tp_size):
            depth = slice(part * feats, (part + 1) * feats)
            normed[:count, depth] = (
                table[part].astype(F32) * scale_back * norm_gain[:, depth]
            ).astype(BF16)

        @pl.loop(0, units // unit_tile)
        def _(tile):
            cols = pl.ds(pl.multiple_of(tile * unit_tile, unit_tile), unit_tile)
            pre_gate = jnp.dot(normed[:count], gate[:, cols], preferred_element_type=F32)
            pre_up = jnp.dot(normed[:count], up[:, cols], preferred_element_type=F32)
            capped = jnp.minimum(pre_gate, CLAMP_LIMIT)
            linear = jnp.clip(pre_up, -CLAMP_LIMIT, CLAMP_LIMIT)
            value = capped * jax.nn.sigmoid(SWISH_ALPHA * capped) * (linear + 1.0)
            hidden[parity, :, cols] = value.astype(BF16)

        hidden_copy(hidden, index, parity).start()

    def far_up(group):
        collect(far_rows.at[group], row_send.at[group], row_recv.at[group])
        run_up(far_rows.at[group], far_hidden.at[group], rows, group)

    def near_up():
        pair_wait()
        run_up(near_rows, near_hidden, near_count, groups)

    def sum_copy(group, step):
        target = lax.rem(chip + step, chips)
        return remote(
            part_send.at[group, step - 1],
            part_recv.at[group, step - 1],
            sum_send.at[group, step - 1],
            sum_recv.at[group, step - 1],
            beside(target * 2 + parity),
        )

    def part_sum(hidden, block, cols):
        value = 0.0
        for core in range(2):
            value += jnp.dot(
                hidden[core],
                down_part[block, core * units : (core + 1) * units, cols],
                preferred_element_type=F32,
            )
        return value

    def column_loop(body):
        @pl.loop(0, columns // column_tile)
        def _(tile):
            body(pl.ds(pl.multiple_of(tile * column_tile, column_tile), column_tile))

    def down_ready():
        weights[3].wait()
        for step in range(1, chips):
            source = lax.rem(chip + step, chips)

            @pl.loop(0, pieces)
            def _(index):
                remote(
                    down_part.at[source, pl.ds(index * chunk, chunk)],
                    down_part.at[source, pl.ds(index * chunk, chunk)],
                    down_send.at[step - 1, index],
                    down_recv.at[source, index],
                    beside(sibling),
                ).wait_recv()

    def far_down(group):
        hidden_copy(far_hidden.at[group], group, 1 - parity).wait_recv()
        for step in range(1, chips):
            def outward(cols):
                part_send[group, step - 1, :, cols] = part_sum(
                    far_hidden.at[group], lax.rem(chip + step, chips), cols
                ).astype(BF16)

            column_loop(outward)
            sum_copy(group, step).start()

        def inward(cols):
            far_sum[group, :, cols] = part_sum(far_hidden.at[group], chip, cols)

        column_loop(inward)

    def near_return(place, block):
        return remote(
            near_result.at[block, pl.ds(place * cap, cap)],
            near_back.at[block, pl.ds(place * cap, cap)],
            near_ret_send.at[place, block],
            near_ret_recv.at[place, block],
            near_at(place),
        )

    def near_down():
        hidden_copy(near_hidden, groups, 1 - parity).wait_recv()
        for step in range(1, chips + 1):
            block = lax.rem(chip + step, chips)

            def store(cols):
                near_result[block, :, cols] = part_sum(near_hidden, block, cols).astype(BF16)

            column_loop(store)

            @pl.loop(1, reach)
            def _(place):
                near_return(place, block).start()

            near_back[block, pl.ds(0, cap), :] = near_result[block, pl.ds(0, cap), :]

    def give_back(place):
        return remote(
            far_result.at[place // span, pl.ds(lax.rem(place, span) * cap, cap)],
            far_back.at[place // span, pl.ds(lax.rem(place, span) * cap, cap)],
            far_ret_send.at[place],
            far_ret_recv.at[place],
            far_at(place),
        )

    def finish(group):
        value = far_sum[group]
        for step in range(1, chips):
            sum_copy(group, step).wait_recv()
            value += part_recv[group, step - 1].astype(F32)
        far_result[group] = value.astype(BF16)
        for place in range(span):
            give_back(group * span + place).start()

    spread_rows(0)
    pair_rows()
    weights[1].wait()
    weights[2].wait()
    near_up()

    @pl.loop(0, groups + 2)
    def _(turn):
        @pl.when(turn < groups - 1)
        def _():
            spread_rows(turn + 1)

        @pl.when(turn < groups)
        def _():
            far_up(turn)

        @pl.when(turn == 1)
        def _():
            down_ready()

        @pl.when(turn >= 2)
        def _():
            finish(turn - 2)

        @pl.when((turn >= 1) & (turn < groups + 1))
        def _():
            far_down(turn - 1)

        @pl.when(turn == 1)
        def _():
            near_down()

    def routed_sum(first, count, table):
        portion = 0.0
        for k, held in enumerate(slots_of(first, count)):
            portion += jnp.where(held, shares[k : k + 1], 0.0)
        coarse = portion.astype(BF16)
        fine = (portion - coarse.astype(F32)).astype(BF16)
        value = 0.0
        for part in (coarse, fine):
            value += lax.dot_general(
                part, table, (((0,), (0,)), ((), ())), preferred_element_type=F32
            )
        return value

    def share_copy(step):
        target = lax.rem(chip + step, chips)
        return remote(
            share_send.at[step - 1],
            share_recv.at[step - 1],
            share_send_sem.at[step - 1],
            share_recv_sem.at[step - 1],
            beside(target * 2 + parity),
        )

    for step in range(1, chips + 1):
        block = lax.rem(chip + step, chips)

        @pl.loop(1, reach)
        def _(place):
            near_return(place, block).wait_recv()

        if step < chips:
            share_send[step - 1] = routed_sum(0, near_count, near_back[block]).astype(BF16)
            share_copy(step).start()
        else:
            sums[...] = mixer[chip].astype(F32) + routed_sum(0, near_count, near_back[chip])

    @pl.loop(0, groups)
    def _(group):
        for place in range(span):
            give_back(group * span + place).wait_recv()
        sums[...] += routed_sum(near_count + group * rows, rows, far_back[group])

    for step in range(1, chips):
        share_copy(step).wait_recv()
        sums[...] += share_recv[step - 1].astype(F32)
    updated[...] = sums[...].astype(BF16)

    @pl.loop(0, pair + 1)
    def _(back):
        block = me - 2 * back

        @pl.when(pair < pairs - 1)
        def _():
            hand_on(block, along_send, back, me + 2).wait_send()

        @pl.when((back > 0) | (side == 0))
        def _():
            hand_on(block, across_send, back, other).wait_send()

    for step in range(1, chips):
        @pl.loop(0, pieces)
        def _(index):
            down_piece(step, index).wait_send()

    for head in range(heads):
        settle(heads_all.at[head], att_send.at[head], att_recv.at[head])

    for step in range(1, chips):
        mix_copy(step).wait_send()
        share_copy(step).wait_send()

    @pl.loop(0, reach)
    def _(place):
        far_dispatch(place).wait_send()
        give_back(place).wait_send()

    for source in range(chips):
        pair_copy(source).wait_send()

        @pl.loop(1, reach)
        def _(place):
            near_dispatch(place, source).wait_send()
            near_return(place, source).wait_send()

    hidden_copy(near_hidden, groups, parity).wait_send()

    @pl.loop(0, groups)
    def _(group):
        settle(far_rows.at[group], row_send.at[group], row_recv.at[group])
        hidden_copy(far_hidden.at[group], group, parity).wait_send()
        for step in range(1, chips):
            sum_copy(group, step).wait_send()


def local(
    residual,
    queries,
    key_rows,
    value_rows,
    diff_scale,
    head_gain,
    out_weight,
    norm_gain,
    gate_weight,
    up_weight,
    down_weight,
    expert_ids,
    route_logit,
):
    sp_size = lax.axis_size("sp")
    tp_size = lax.axis_size("tp")
    tokens, heads, width = value_rows.shape
    feats = residual.shape[1]
    tops = expert_ids.shape[1]
    cap = -(-(2 * tokens * tops // sp_size) // 16) * 16
    reach = sp_size // 2
    groups = math.gcd(reach, 4)
    rows = reach // groups * cap
    near_count = reach * cap
    units = gate_weight.shape[2]
    chips = tp_size // 2
    peers = max(chips - 1, 1)
    pieces = 16
    early = 13
    dma = pltpu.SemaphoreType.DMA
    vmem = pl.BlockSpec(memory_space=pltpu.VMEM)
    hbm = pl.BlockSpec(memory_space=pl.ANY)
    return pl.pallas_call(
        functools.partial(layer_kernel, sp_size, tp_size, groups, cap, early),
        out_shape=jax.ShapeDtypeStruct((tokens, feats), BF16),
        in_specs=[
            hbm,
            hbm,
            hbm,
            hbm,
            pl.BlockSpec(memory_space=pltpu.SMEM),
            vmem,
            hbm,
            vmem,
            hbm,
            hbm,
            hbm,
            vmem,
            vmem,
        ],
        out_specs=vmem,
        scratch_shapes=[
            pltpu.VMEM((tokens, feats), BF16),
            pltpu.VMEM((3, tokens, heads, width), BF16),
            pltpu.VMEM((2, heads, tokens, width), BF16),
            pltpu.VMEM((sp_size, 2, heads, tokens, width), BF16),
            pltpu.VMEM((heads * 2, 1, tokens), F32),
            pltpu.VMEM((heads * 2, width + 16, tokens), F32),
            pltpu.VMEM((heads, tp_size, tokens, width), BF16),
            pltpu.VMEM(out_weight.shape, BF16),
            pltpu.VMEM((chips, tokens, feats), BF16),
            pltpu.VMEM((tops, tokens), jnp.int32),
            pltpu.VMEM((reach, chips, cap, feats), BF16),
            pltpu.VMEM((reach, cap, feats), BF16),
            pltpu.VMEM((tp_size, near_count, feats), BF16),
            pltpu.VMEM((groups, tp_size, rows, feats), BF16),
            pltpu.VMEM((near_count, tp_size * feats), BF16),
            pltpu.VMEM((2, near_count, units), BF16),
            pltpu.VMEM((groups, 2, rows, units), BF16),
            pltpu.VMEM((chips, 2 * units, feats), BF16),
            pltpu.VMEM((tokens, feats), F32),
            pltpu.VMEM((groups, rows, feats), F32),
            pltpu.VMEM((groups, peers, rows, feats), BF16),
            pltpu.VMEM((groups, peers, rows, feats), BF16),
            pltpu.VMEM((chips, near_count, feats), BF16),
            pltpu.VMEM((groups, rows, feats), BF16),
            pltpu.VMEM((chips, near_count, feats), BF16),
            pltpu.VMEM((groups, rows, feats), BF16),
            pltpu.VMEM((peers, tokens, feats), BF16),
            pltpu.VMEM((peers, tokens, feats), BF16),
            pltpu.VMEM(gate_weight.shape[1:], BF16),
            pltpu.VMEM(up_weight.shape[1:], BF16),
            dma((5,)),
            dma((3,)),
            dma((sp_size,)),
            dma((sp_size,)),
            dma((sp_size,)),
            dma((peers, pieces)),
            dma((chips, pieces)),
            dma((heads, tp_size)),
            dma((heads, tp_size)),
            dma((peers,)),
            dma((chips,)),
            dma((reach, chips)),
            dma((reach, chips)),
            dma((reach,)),
            dma((reach,)),
            dma((chips,)),
            dma((chips,)),
            dma((groups, tp_size)),
            dma((groups, tp_size)),
            dma((groups + 1,)),
            dma((groups + 1,)),
            dma((groups, peers)),
            dma((groups, peers)),
            dma((reach, chips)),
            dma((reach, chips)),
            dma((reach,)),
            dma((reach,)),
            dma((peers,)),
            dma((peers,)),
        ],
        compiler_params=pltpu.CompilerParams(
            collective_id=0, has_side_effects=True, vmem_limit_bytes=56 * 1024 * 1024
        ),
    )(
        residual,
        queries,
        key_rows,
        value_rows,
        diff_scale,
        head_gain[None],
        out_weight,
        norm_gain[None],
        gate_weight[0],
        up_weight[0],
        down_weight[0],
        expert_ids.T,
        route_logit.T,
    )


def solution(mesh):
    return jax.shard_map(
        local,
        mesh=mesh,
        in_specs=(
            P("sp", "tp"),
            P("sp", "tp", None),
            P("sp", "tp", None),
            P("sp", "tp", None),
            P("tp"),
            P(),
            P(None, "tp"),
            P(),
            P("sp", None, "tp"),
            P("sp", None, "tp"),
            P("sp", None, "tp"),
            P("sp", None),
            P("sp", None),
        ),
        out_specs=P("sp", "tp"),
        check_vma=False,
    )
```

```python
import functools
import math

import jax
import jax.numpy as jnp
from jax import lax
from jax.experimental import pallas as pl
from jax.experimental.pallas import tpu as pltpu
from jax.sharding import PartitionSpec as P

D = 2048
QK = 64
SPAN = 64


NORM_EPS = 1e-05
CLAMP_LIMIT = 7.0
SWISH_ALPHA = 1.702
HEAD_KEEP = 0.8
NEG_FILL = -1e30
MESH = pl.DeviceIdType.MESH
F32 = jnp.float32
BF16 = jnp.bfloat16


def layer_kernel(
    sp_size,
    tp_size,
    groups,
    cap,
    early,
    residual_hbm,
    query_hbm,
    key_hbm,
    value_hbm,
    diff_scale,
    head_gain,
    out_hbm,
    norm_gain,
    gate_hbm,
    up_hbm,
    down_hbm,
    expert_ids,
    route_logit,
    updated,
    residual,
    raw,
    scaled,
    blocks,
    peak,
    accum,
    heads_all,
    out_w,
    mixer,
    places,
    near_out,
    far_out,
    near_rows,
    far_rows,
    normed,
    near_hidden,
    far_hidden,
    down_part,
    own_sum,
    far_sum,
    part_send,
    part_recv,
    near_result,
    far_result,
    near_back,
    far_back,
    share_send,
    share_recv,
    gate,
    up,
    weight_sem,
    raw_sem,
    along_send,
    across_send,
    kv_recv,
    rest_send,
    rest_recv,
    down_send,
    down_recv,
    att_send,
    att_recv,
    mix_send,
    mix_recv,
    near_send,
    near_recv,
    far_send,
    far_recv,
    pair_send,
    pair_recv,
    row_send,
    row_recv,
    hid_send,
    hid_recv,
    sum_send,
    sum_recv,
    near_ret_send,
    near_ret_recv,
    far_ret_send,
    far_ret_recv,
    share_send_sem,
    share_recv_sem,
):
    me = lax.axis_index("sp")
    rank = lax.axis_index("tp")
    parity = lax.rem(rank, 2)
    sibling = rank + 1 - 2 * parity
    chips = tp_size // 2
    chip = rank // 2
    reach = sp_size // 2
    half_of = me // reach
    spot = lax.rem(me, reach)
    span = reach // groups
    ahead = (groups + 1) // 2
    rows = span * cap
    near_count = reach * cap
    tokens, heads, width = query_hbm.shape
    feats = residual.shape[1]
    units = gate.shape[1]
    columns = feats
    tops = expert_ids.shape[0]

    def at(index):
        return {"sp": index, "tp": rank}

    def beside(target):
        return {"sp": me, "tp": target}

    def peer_rank(step):
        return lax.rem(chip + step, chips) * 2 + parity

    def remote(src, dst, send, recv, device):
        return pltpu.make_async_remote_copy(
            src_ref=src,
            dst_ref=dst,
            send_sem=send,
            recv_sem=recv,
            device_id=device,
            device_id_type=MESH,
        )

    raw_loads = [
        pltpu.make_async_copy(source, raw.at[i], raw_sem.at[i])
        for i, source in enumerate((key_hbm, value_hbm, query_hbm))
    ]
    for copy in raw_loads:
        copy.start()
    pieces = down_send.shape[1]
    chunk = 2 * units // pieces
    weights = [
        pltpu.make_async_copy(out_hbm, out_w, weight_sem.at[0]),
        pltpu.make_async_copy(gate_hbm, gate, weight_sem.at[1]),
        pltpu.make_async_copy(up_hbm, up, weight_sem.at[2]),
        pltpu.make_async_copy(
            down_hbm.at[pl.ds(chip * 2 * units, 2 * units)], down_part.at[chip], weight_sem.at[3]
        ),
        pltpu.make_async_copy(residual_hbm, residual, weight_sem.at[4]),
    ]

    barrier = pltpu.get_barrier_semaphore()
    for step in range(1, sp_size):
        pl.semaphore_signal(
            barrier, inc=1, device_id=at(lax.rem(me + step, sp_size)), device_id_type=MESH
        )
    for step in range(1, chips):
        pl.semaphore_signal(barrier, inc=1, device_id=beside(peer_rank(step)), device_id_type=MESH)
    pl.semaphore_signal(barrier, inc=1, device_id=beside(sibling), device_id_type=MESH)

    accum[...] = jnp.zeros(accum.shape, F32)
    peak[...] = jnp.full(peak.shape, NEG_FILL, F32)

    spare = -(-sp_size // 16) * 16
    names = lax.broadcasted_iota(jnp.int32, (spare, tokens), 0)
    named = [names == expert_ids[k : k + 1] for k in range(tops)]
    both = functools.reduce(jnp.logical_or, named).astype(F32).astype(BF16)
    before = (
        lax.broadcasted_iota(jnp.int32, (tokens, tokens), 0)
        < lax.broadcasted_iota(jnp.int32, (tokens, tokens), 1)
    ).astype(F32).astype(BF16)
    earlier = jnp.dot(both, before, preferred_element_type=F32)
    peak_logit = jnp.max(route_logit[...], axis=0, keepdims=True)
    shares = jnp.exp(route_logit[...] - peak_logit)
    shares = shares / jnp.sum(shares, axis=0, keepdims=True)
    for k in range(tops):
        order = jnp.sum(jnp.where(named[k], earlier, 0.0), axis=0, keepdims=True)
        expert = expert_ids[k : k + 1]
        apart = jnp.where(expert // reach == half_of, 0, reach)
        step_of = lax.rem(spot + reach - lax.rem(expert, reach), reach) + apart
        places[k : k + 1] = step_of * cap + order.astype(jnp.int32)

    for i in range(2):
        raw_loads[i].wait()
        blocks[me, :, i] = jnp.transpose(raw[i], (1, 0, 2))
    raw_loads[2].wait()
    low = lax.broadcasted_iota(jnp.int32, (heads, tokens, width), 2) < QK
    query = jnp.transpose(raw[2], (1, 0, 2)).astype(F32) * QK ** (-0.5)
    scaled[0] = jnp.where(low, query, 0.0).astype(BF16)
    scaled[1] = jnp.where(low, 0.0, query).astype(BF16)

    pl.semaphore_wait(barrier, sp_size - 1 + chips)

    def down_piece(step, piece):
        target = lax.rem(chip + step, chips)
        return remote(
            down_hbm.at[pl.ds(target * 2 * units + piece * chunk, chunk)],
            down_part.at[chip, pl.ds(piece * chunk, chunk)],
            down_send.at[step - 1, piece],
            down_recv.at[chip, piece],
            beside(target * 2 + parity),
        )

    def send_down(first, last):
        for step in range(1, chips):
            @pl.loop(first, last)
            def _(piece):
                down_piece(step, piece).start()

    pairs = sp_size // 2
    pair = me // 2
    side = lax.rem(me, 2)
    other = me + 1 - 2 * side

    def hand_on(block, send, back, target):
        return remote(
            blocks.at[block], blocks.at[block], send.at[back], kv_recv.at[block], at(target)
        )

    top = pairs - 1
    kept = heads // 2 if heads % 2 == 0 and pairs > 1 else heads

    def kept_part(block, send, back, target):
        part = blocks.at[block, pl.ds(0, kept)]
        return remote(part, part, send.at[back], kv_recv.at[block], at(target))

    def rest_part(target):
        part = blocks.at[0, pl.ds(kept, heads - kept)]
        return remote(part, part, rest_send, rest_recv, at(target))

    def attend(block, masked):
        if masked:
            key = block * tokens + lax.broadcasted_iota(jnp.int32, (tokens, tokens), 0)
            query = me * tokens + lax.broadcasted_iota(jnp.int32, (tokens, tokens), 1)
            visible = key // SPAN <= query // SPAN
        for head in range(heads):
            value = jnp.concatenate(
                [jnp.transpose(blocks[block, head, 1]), jnp.ones((16, tokens), BF16)], axis=0
            )
            for half in range(2):
                scores = lax.dot_general(
                    blocks[block, head, 0],
                    scaled[half, head],
                    (((1,), (1,)), ((), ())),
                    preferred_element_type=F32,
                )
                if masked:
                    scores = jnp.where(visible, scores, NEG_FILL)
                index = head * 2 + half
                old = peak[index]
                new = jnp.maximum(old, jnp.max(scores, axis=0, keepdims=True))
                exps = jnp.exp(scores - new)
                if masked:
                    exps = jnp.where(visible, exps, 0.0)
                peak[index] = new
                accum[index] = accum[index] * jnp.exp(old - new) + jnp.dot(
                    value, exps.astype(BF16), preferred_element_type=F32
                )

    plain_blocks = tokens % SPAN == 0

    @pl.loop(0, pair + 2)
    def _(back):
        @pl.when(back <= pair)
        def _():
            block = me - 2 * back

            @pl.when(back > 0)
            def _():
                hand_on(block, across_send, back, other).wait_recv()

            @pl.when(pair < pairs - 1)
            def _():
                hand_on(block, along_send, back, me + 2).start()

            cut = (pair == top) & (side == 0) & (back == pair) & (kept < heads)

            @pl.when(((back > 0) | (side == 0)) & jnp.logical_not(cut))
            def _():
                hand_on(block, across_send, back, other).start()

            @pl.when(cut)
            def _():
                kept_part(block, across_send, back, other).start()

        @pl.when(back == 0)
        def _():
            send_down(0, early)
            for copy in weights:
                copy.start()
            attend(me, True)

        second = other - 2 * (back - 1)
        use_second = (back >= 2) | ((back == 1) & (side == 1))

        @pl.loop(0, 2)
        def _(which):
            parted = (me == sp_size - 1) & (second == 0) & (kept < heads)

            @pl.when((which == 1) & use_second & jnp.logical_not(parted))
            def _():
                hand_on(second, across_send, 0, other).wait_recv()

            if kept < heads:
                @pl.when((which == 1) & use_second & parted)
                def _():
                    kept_part(second, across_send, 0, other).wait_recv()
                    rest_part(other).wait_recv()

                @pl.when((which == 1) & use_second & (me == sp_size - 3) & (second == 0))
                def _():
                    rest_part(me + 2).start()

            @pl.when(((which == 0) & (back > 0) & (back <= pair)) | ((which == 1) & use_second))
            def _():
                attend(jnp.where(which == 0, me - 2 * back, second), not plain_blocks)

    def piece(buffer, send, recv, owner, target, send_slot):
        return remote(
            buffer.at[owner],
            buffer.at[owner],
            send.at[send_slot],
            recv.at[owner],
            beside(target),
        )

    def spread(buffer, send, recv):
        for step in range(1, chips):
            target = peer_rank(step)
            piece(buffer, send, recv, rank, target, target).start()
        piece(buffer, send, recv, rank, sibling, sibling).start()

    def forward(buffer, send, recv, step):
        owner = peer_rank(step)
        onward = piece(buffer, send, recv, owner, sibling, owner + 1 - 2 * parity)
        onward.wait_recv()
        onward.start()

    def collect(buffer, send, recv):
        for step in range(chips):
            owner = peer_rank(step) + 1 - 2 * parity
            piece(buffer, send, recv, owner, sibling, sibling).wait_recv()

    def settle(buffer, send, recv):
        for step in range(1, chips):
            target = peer_rank(step)
            piece(buffer, send, recv, rank, target, target).wait_send()
            piece(buffer, send, recv, target, sibling, target + 1 - 2 * parity).wait_send()
        piece(buffer, send, recv, rank, sibling, sibling).wait_send()

    for head in range(heads):
        shrink = [
            1.0 / accum[index, width : width + 1] for index in (head * 2, head * 2 + 1)
        ]
        mixture = (
            accum[head * 2, :width] * shrink[0]
            - accum[head * 2 + 1, :width] * (diff_scale[head] * shrink[1])
        )
        scale_back = lax.rsqrt(jnp.mean(mixture * mixture, axis=0, keepdims=True) + NORM_EPS)
        heads_all[head, rank] = (
            jnp.transpose(mixture * scale_back) * head_gain[...] * HEAD_KEEP
        ).astype(BF16)
        spread(heads_all.at[head], att_send.at[head], att_recv.at[head])
    weights[0].wait()
    weights[4].wait()

    def project(owner):
        return jnp.dot(
            jnp.concatenate([heads_all[head, owner] for head in range(heads)], axis=1),
            out_w[pl.ds(pl.multiple_of(owner * heads * width, heads * width), heads * width)],
            preferred_element_type=F32,
        )

    sums = updated
    sums[...] = residual[...].astype(F32) + project(rank)
    for head in range(heads):
        for step in range(1, chips):
            forward(heads_all.at[head], att_send.at[head], att_recv.at[head], step)

    def from_sibling(step):
        owner = peer_rank(step) + 1 - 2 * parity
        for head in range(heads):
            piece(
                heads_all.at[head], att_send.at[head], att_recv.at[head], owner, sibling, sibling
            ).wait_recv()
        return project(owner)

    send_down(early, early + 1)
    sums[...] += from_sibling(0)
    for step in range(1, chips):
        sums[...] += project(peer_rank(step))
    for step in range(1, chips):
        sums[...] += from_sibling(step)
    mixer[chip] = sums[...].astype(BF16)

    def mix_copy(step):
        target = lax.rem(chip + step, chips)
        return remote(
            mixer.at[chip],
            mixer.at[chip],
            mix_send.at[step - 1],
            mix_recv.at[chip],
            beside(target * 2 + parity),
        )

    for step in range(1, chips):
        mix_copy(step).start()

    def slots_of(first, count):
        slot = first + lax.broadcasted_iota(jnp.int32, (count, tokens), 0)
        return [slot == places[k : k + 1] for k in range(tops)]

    def chosen_rows(step, source):
        held = functools.reduce(jnp.logical_or, slots_of(step * cap, cap))
        return jnp.dot(
            held.astype(F32).astype(BF16), mixer[source], preferred_element_type=F32
        ).astype(BF16)

    def near_at(place):
        return at(half_of * reach + lax.rem(spot + reach + place, reach))

    def far_at(place):
        return at((1 - half_of) * reach + lax.rem(spot + reach + place, reach))

    def far_dispatch(place):
        return remote(
            far_out.at[place],
            far_rows.at[place // span, rank, pl.ds(lax.rem(place, span) * cap, cap)],
            far_send.at[place],
            far_recv.at[place],
            far_at(-place),
        )

    def near_dispatch(place, source):
        return remote(
            near_out.at[place, source],
            near_rows.at[source * 2 + parity, pl.ds(place * cap, cap)],
            near_send.at[place, source],
            near_recv.at[place, source],
            near_at(-place),
        )

    def send_near(source):
        near_rows[source * 2 + parity, pl.ds(0, cap), :] = chosen_rows(0, source)

        @pl.loop(1, reach)
        def _(place):
            near_out[place, source] = chosen_rows(place, source)
            near_dispatch(place, source).start()

    def send_far(first, last):
        @pl.loop(first, last)
        def _(place):
            far_out[place] = chosen_rows(reach + place, chip)
            far_dispatch(place).start()

    send_far(0, span)
    send_near(chip)
    send_far(span, span * ahead)
    for step in range(1, chips):
        source = lax.rem(chip + step, chips)
        remote(
            mixer.at[source],
            mixer.at[source],
            mix_send.at[step - 1],
            mix_recv.at[source],
            beside(sibling),
        ).wait_recv()
        if step == 1:
            send_down(early + 1, early + 2)
        send_near(source)
    send_far(span * ahead, reach)

    unit_tile = math.gcd(units, 256)
    column_tile = math.gcd(columns, 256)

    def spread_rows(group):
        for place in range(span):
            remote(
                far_out.at[0],
                far_rows.at[group, rank, pl.ds(place * cap, cap)],
                far_send.at[group * span + place],
                far_recv.at[group * span + place],
                beside(sibling),
            ).wait_recv()
        spread(far_rows.at[group], row_send.at[group], row_recv.at[group])

    def pair_copy(source):
        return remote(
            near_rows.at[source * 2 + parity],
            near_rows.at[source * 2 + parity],
            pair_send.at[source],
            pair_recv.at[source],
            beside(sibling),
        )

    def pair_rows():
        for step in range(chips):
            source = lax.rem(chip + step, chips)

            @pl.loop(1, reach)
            def _(place):
                remote(
                    near_out.at[0, 0],
                    near_rows.at[source * 2 + parity, pl.ds(place * cap, cap)],
                    near_send.at[place, source],
                    near_recv.at[place, source],
                    beside(sibling),
                ).wait_recv()

            pair_copy(source).start()

    def pair_wait():
        for step in range(chips):
            source = lax.rem(chip + step, chips)
            remote(
                near_rows.at[source * 2 + 1 - parity],
                near_rows.at[source * 2 + 1 - parity],
                pair_send.at[source],
                pair_recv.at[source],
                beside(sibling),
            ).wait_recv()

    def hidden_copy(hidden, index, core):
        return remote(
            hidden.at[core],
            hidden.at[core],
            hid_send.at[index],
            hid_recv.at[index],
            beside(sibling),
        )

    def run_up(table, hidden, count, index, beat=None):
        square = 0.0
        for part in range(tp_size):
            value = table[part].astype(F32)
            square += jnp.sum(value * value, axis=-1, keepdims=True)
        scale_back = lax.rsqrt(square / (tp_size * feats) + NORM_EPS)
        for part in range(tp_size):
            depth = slice(part * feats, (part + 1) * feats)
            normed[:count, depth] = (
                table[part].astype(F32) * scale_back * norm_gain[:, depth]
            ).astype(BF16)

        @pl.loop(0, units // unit_tile)
        def _(tile):
            cols = pl.ds(pl.multiple_of(tile * unit_tile, unit_tile), unit_tile)
            pre_gate = jnp.dot(normed[:count], gate[:, cols], preferred_element_type=F32)
            pre_up = jnp.dot(normed[:count], up[:, cols], preferred_element_type=F32)
            capped = jnp.minimum(pre_gate, CLAMP_LIMIT)
            linear = jnp.clip(pre_up, -CLAMP_LIMIT, CLAMP_LIMIT)
            value = capped * jax.nn.sigmoid(SWISH_ALPHA * capped) * (linear + 1.0)
            hidden[parity, :, cols] = value.astype(BF16)
            if beat is not None:
                beat(tile)

        hidden_copy(hidden, index, parity).start()

    def hand_over(group):
        for step in range(1, chips):
            forward(far_rows.at[group], row_send.at[group], row_recv.at[group], step)

    def far_up(group, beat=None):
        collect(far_rows.at[group], row_send.at[group], row_recv.at[group])
        run_up(far_rows.at[group], far_hidden.at[group], rows, group, beat)

    def near_up(beat):
        pair_wait()
        run_up(near_rows, near_hidden, near_count, groups, beat)

    def sum_copy(group, step):
        target = lax.rem(chip + step, chips)
        return remote(
            part_send.at[group, step - 1],
            part_recv.at[group, step - 1],
            sum_send.at[group, step - 1],
            sum_recv.at[group, step - 1],
            beside(target * 2 + parity),
        )

    def part_sum(hidden, block, cols):
        value = 0.0
        for core in range(2):
            value += jnp.dot(
                hidden[core],
                down_part[block, core * units : (core + 1) * units, cols],
                preferred_element_type=F32,
            )
        return value

    def column_loop(body):
        @pl.loop(0, columns // column_tile)
        def _(tile):
            body(pl.ds(pl.multiple_of(tile * column_tile, column_tile), column_tile))

    def down_ready():
        weights[3].wait()
        for step in range(1, chips):
            source = lax.rem(chip + step, chips)

            @pl.loop(0, pieces)
            def _(index):
                remote(
                    down_part.at[source, pl.ds(index * chunk, chunk)],
                    down_part.at[source, pl.ds(index * chunk, chunk)],
                    down_send.at[step - 1, index],
                    down_recv.at[source, index],
                    beside(sibling),
                ).wait_recv()

    def far_down(group):
        hidden_copy(far_hidden.at[group], group, 1 - parity).wait_recv()
        for step in range(1, chips):
            def outward(cols):
                part_send[group, step - 1, :, cols] = part_sum(
                    far_hidden.at[group], lax.rem(chip + step, chips), cols
                ).astype(BF16)

            column_loop(outward)
            sum_copy(group, step).start()

        def inward(cols):
            far_sum[group, :, cols] = part_sum(far_hidden.at[group], chip, cols)

        column_loop(inward)

    def near_return(place, block):
        return remote(
            near_result.at[block, pl.ds(place * cap, cap)],
            near_back.at[block, pl.ds(place * cap, cap)],
            near_ret_send.at[place, block],
            near_ret_recv.at[place, block],
            near_at(place),
        )

    def near_down():
        hidden_copy(near_hidden, groups, 1 - parity).wait_recv()
        for step in range(1, chips + 1):
            block = lax.rem(chip + step, chips)

            def store(cols):
                near_result[block, :, cols] = part_sum(near_hidden, block, cols).astype(BF16)

            column_loop(store)

            @pl.loop(1, reach)
            def _(place):
                near_return(place, block).start()

            near_back[block, pl.ds(0, cap), :] = near_result[block, pl.ds(0, cap), :]

    def give_back(place):
        return remote(
            far_result.at[place // span, pl.ds(lax.rem(place, span) * cap, cap)],
            far_back.at[place // span, pl.ds(lax.rem(place, span) * cap, cap)],
            far_ret_send.at[place],
            far_ret_recv.at[place],
            far_at(place),
        )

    def finish(group):
        value = far_sum[group]
        for step in range(1, chips):
            sum_copy(group, step).wait_recv()
            value += part_recv[group, step - 1].astype(F32)
        far_result[group] = value.astype(BF16)
        for place in range(span):
            give_back(group * span + place).start()

    def at_tiles(acts):
        def beat(tile):
            for number, act in acts:
                pl.when(tile == number)(act)

        return beat

    last_tile = units // unit_tile - 1
    first_part = list(range(ahead))
    second_part = list(range(ahead, groups))

    def second_out():
        for group in second_part:
            spread_rows(group)

    def first_done():
        for group in first_part:
            finish(group)

    weights[1].wait()
    weights[2].wait()
    for group in first_part:
        spread_rows(group)
    pair_rows()
    send_down(early + 2, pieces)
    for group in first_part:
        hand_over(group)
    for group in first_part:
        far_up(group)
    near_up(at_tiles([(0, second_out)]))
    down_ready()
    for group in first_part:
        far_down(group)
    for group in second_part:
        hand_over(group)
        far_up(group, at_tiles([(last_tile, first_done)]))
    for group in second_part:
        far_down(group)
    near_down()
    for group in second_part:
        finish(group)

    def routed_sum(first, count, table):
        portion = 0.0
        for k, held in enumerate(slots_of(first, count)):
            portion += jnp.where(held, shares[k : k + 1], 0.0)
        coarse = portion.astype(BF16)
        fine = (portion - coarse.astype(F32)).astype(BF16)
        value = 0.0
        for part in (coarse, fine):
            value += lax.dot_general(
                part, table, (((0,), (0,)), ((), ())), preferred_element_type=F32
            )
        return value

    def share_copy(step):
        target = lax.rem(chip + step, chips)
        return remote(
            share_send.at[step - 1],
            share_recv.at[step - 1],
            share_send_sem.at[step - 1],
            share_recv_sem.at[step - 1],
            beside(target * 2 + parity),
        )

    for step in range(1, chips + 1):
        block = lax.rem(chip + step, chips)

        @pl.loop(1, reach)
        def _(place):
            near_return(place, block).wait_recv()

        if step < chips:
            share_send[step - 1] = routed_sum(0, near_count, near_back[block]).astype(BF16)
            share_copy(step).start()
        else:
            sums[...] = mixer[chip].astype(F32) + routed_sum(0, near_count, near_back[chip])

    @pl.loop(0, groups)
    def _(group):
        for place in range(span):
            give_back(group * span + place).wait_recv()
        sums[...] += routed_sum(near_count + group * rows, rows, far_back[group])

    for step in range(1, chips):
        share_copy(step).wait_recv()
        sums[...] += share_recv[step - 1].astype(F32)

    @pl.loop(0, pair + 1)
    def _(back):
        block = me - 2 * back

        @pl.when(pair < pairs - 1)
        def _():
            hand_on(block, along_send, back, me + 2).wait_send()

        cut = (pair == top) & (side == 0) & (back == pair) & (kept < heads)

        @pl.when(((back > 0) | (side == 0)) & jnp.logical_not(cut))
        def _():
            hand_on(block, across_send, back, other).wait_send()

        @pl.when(cut)
        def _():
            kept_part(block, across_send, back, other).wait_send()

    if kept < heads:
        @pl.when(me == sp_size - 3)
        def _():
            rest_part(me + 2).wait_send()

    for step in range(1, chips):
        @pl.loop(0, pieces)
        def _(index):
            down_piece(step, index).wait_send()

    for head in range(heads):
        settle(heads_all.at[head], att_send.at[head], att_recv.at[head])

    for step in range(1, chips):
        mix_copy(step).wait_send()
        share_copy(step).wait_send()

    @pl.loop(0, reach)
    def _(place):
        far_dispatch(place).wait_send()
        give_back(place).wait_send()

    for source in range(chips):
        pair_copy(source).wait_send()

        @pl.loop(1, reach)
        def _(place):
            near_dispatch(place, source).wait_send()
            near_return(place, source).wait_send()

    hidden_copy(near_hidden, groups, parity).wait_send()

    @pl.loop(0, groups)
    def _(group):
        settle(far_rows.at[group], row_send.at[group], row_recv.at[group])
        hidden_copy(far_hidden.at[group], group, parity).wait_send()
        for step in range(1, chips):
            sum_copy(group, step).wait_send()


def local(
    residual,
    queries,
    key_rows,
    value_rows,
    diff_scale,
    head_gain,
    out_weight,
    norm_gain,
    gate_weight,
    up_weight,
    down_weight,
    expert_ids,
    route_logit,
):
    sp_size = lax.axis_size("sp")
    tp_size = lax.axis_size("tp")
    tokens, heads, width = value_rows.shape
    feats = residual.shape[1]
    tops = expert_ids.shape[1]
    cap = -(-(2 * tokens * tops // sp_size) // 16) * 16
    reach = sp_size // 2
    groups = math.gcd(reach, 2)
    rows = reach // groups * cap
    near_count = reach * cap
    units = gate_weight.shape[2]
    chips = tp_size // 2
    peers = max(chips - 1, 1)
    pieces = 16
    early = 12
    dma = pltpu.SemaphoreType.DMA
    vmem = pl.BlockSpec(memory_space=pltpu.VMEM)
    hbm = pl.BlockSpec(memory_space=pl.ANY)
    return pl.pallas_call(
        functools.partial(layer_kernel, sp_size, tp_size, groups, cap, early),
        out_shape=jax.ShapeDtypeStruct((tokens, feats), F32),
        in_specs=[
            hbm,
            hbm,
            hbm,
            hbm,
            pl.BlockSpec(memory_space=pltpu.SMEM),
            vmem,
            hbm,
            vmem,
            hbm,
            hbm,
            hbm,
            vmem,
            vmem,
        ],
        out_specs=vmem,
        scratch_shapes=[
            pltpu.VMEM((tokens, feats), BF16),
            pltpu.VMEM((3, tokens, heads, width), BF16),
            pltpu.VMEM((2, heads, tokens, width), BF16),
            pltpu.VMEM((sp_size, heads, 2, tokens, width), BF16),
            pltpu.VMEM((heads * 2, 1, tokens), F32),
            pltpu.VMEM((heads * 2, width + 16, tokens), F32),
            pltpu.VMEM((heads, tp_size, tokens, width), BF16),
            pltpu.VMEM(out_weight.shape, BF16),
            pltpu.VMEM((chips, tokens, feats), BF16),
            pltpu.VMEM((tops, tokens), jnp.int32),
            pltpu.VMEM((reach, chips, cap, feats), BF16),
            pltpu.VMEM((reach, cap, feats), BF16),
            pltpu.VMEM((tp_size, near_count, feats), BF16),
            pltpu.VMEM((groups, tp_size, rows, feats), BF16),
            pltpu.VMEM((near_count, tp_size * feats), BF16),
            pltpu.VMEM((2, near_count, units), BF16),
            pltpu.VMEM((groups, 2, rows, units), BF16),
            pltpu.VMEM((chips, 2 * units, feats), BF16),
            pltpu.VMEM((tokens, feats), F32),
            pltpu.VMEM((groups, rows, feats), F32),
            pltpu.VMEM((groups, peers, rows, feats), BF16),
            pltpu.VMEM((groups, peers, rows, feats), BF16),
            pltpu.VMEM((chips, near_count, feats), BF16),
            pltpu.VMEM((groups, rows, feats), BF16),
            pltpu.VMEM((chips, near_count, feats), BF16),
            pltpu.VMEM((groups, rows, feats), BF16),
            pltpu.VMEM((peers, tokens, feats), BF16),
            pltpu.VMEM((peers, tokens, feats), BF16),
            pltpu.VMEM(gate_weight.shape[1:], BF16),
            pltpu.VMEM(up_weight.shape[1:], BF16),
            dma((5,)),
            dma((3,)),
            dma((sp_size,)),
            dma((sp_size,)),
            dma((sp_size,)),
            dma(()),
            dma(()),
            dma((peers, pieces)),
            dma((chips, pieces)),
            dma((heads, tp_size)),
            dma((heads, tp_size)),
            dma((peers,)),
            dma((chips,)),
            dma((reach, chips)),
            dma((reach, chips)),
            dma((reach,)),
            dma((reach,)),
            dma((chips,)),
            dma((chips,)),
            dma((groups, tp_size)),
            dma((groups, tp_size)),
            dma((groups + 1,)),
            dma((groups + 1,)),
            dma((groups, peers)),
            dma((groups, peers)),
            dma((reach, chips)),
            dma((reach, chips)),
            dma((reach,)),
            dma((reach,)),
            dma((peers,)),
            dma((peers,)),
        ],
        compiler_params=pltpu.CompilerParams(
            collective_id=0, has_side_effects=True, vmem_limit_bytes=56 * 1024 * 1024
        ),
    )(
        residual,
        queries,
        key_rows,
        value_rows,
        diff_scale,
        head_gain[None],
        out_weight,
        norm_gain[None],
        gate_weight[0],
        up_weight[0],
        down_weight[0],
        expert_ids.T,
        route_logit.T,
    ).astype(BF16)


def solution(mesh):
    return jax.shard_map(
        local,
        mesh=mesh,
        in_specs=(
            P("sp", "tp"),
            P("sp", "tp", None),
            P("sp", "tp", None),
            P("sp", "tp", None),
            P("tp"),
            P(),
            P(None, "tp"),
            P(),
            P("sp", None, "tp"),
            P("sp", None, "tp"),
            P("sp", None, "tp"),
            P("sp", None),
            P("sp", None),
        ),
        out_specs=P("sp", "tp"),
        check_vma=False,
    )
```

```python
import functools
import math

import jax
import jax.numpy as jnp
from jax import lax
from jax.experimental import pallas as pl
from jax.experimental.pallas import tpu as pltpu
from jax.sharding import PartitionSpec as P

D = 2048
QK = 64
SPAN = 64


NORM_EPS = 1e-05
CLAMP_LIMIT = 7.0
SWISH_ALPHA = 1.702
HEAD_KEEP = 0.8
NEG_FILL = -1e30
MESH = pl.DeviceIdType.MESH
F32 = jnp.float32
BF16 = jnp.bfloat16


def layer_kernel(
    sp_size,
    tp_size,
    groups,
    cap,
    ext,
    chunk,
    residual_hbm,
    query_hbm,
    key_hbm,
    value_hbm,
    diff_scale,
    head_gain,
    out_hbm,
    norm_gain,
    gate_hbm,
    up_hbm,
    down_hbm,
    expert_ids,
    route_logit,
    updated,
    residual,
    raw,
    scaled,
    blocks,
    peak,
    accum,
    heads_all,
    out_w,
    mixer,
    places,
    near_out,
    far_out,
    near_rows,
    far_rows,
    normed,
    near_hidden,
    far_hidden,
    far_ext,
    near_ext,
    down_part,
    down_ext,
    own_sum,
    far_sum,
    part_send,
    part_recv,
    near_result,
    far_result,
    near_back,
    far_back,
    share_send,
    share_recv,
    gate,
    up,
    weight_sem,
    raw_sem,
    along_send,
    across_send,
    kv_recv,
    rest_send,
    rest_recv,
    down_send,
    down_recv,
    att_send,
    att_recv,
    mix_send,
    mix_recv,
    near_send,
    near_recv,
    far_send,
    far_recv,
    pair_send,
    pair_recv,
    row_send,
    row_recv,
    hid_send,
    hid_recv,
    ext_send,
    ext_recv,
    ext_over_send,
    sum_send,
    sum_recv,
    near_ret_send,
    near_ret_recv,
    far_ret_send,
    far_ret_recv,
    share_send_sem,
    share_recv_sem,
):
    me = lax.axis_index("sp")
    rank = lax.axis_index("tp")
    parity = lax.rem(rank, 2)
    sibling = rank + 1 - 2 * parity
    chips = tp_size // 2
    chip = rank // 2
    reach = sp_size // 2
    half_of = me // reach
    spot = lax.rem(me, reach)
    span = reach // groups
    ahead = (groups + 1) // 2
    rows = span * cap
    near_count = reach * cap
    tokens, heads, width = query_hbm.shape
    feats = residual.shape[1]
    units = gate.shape[1]
    columns = feats
    tops = expert_ids.shape[0]

    def at(index):
        return {"sp": index, "tp": rank}

    def beside(target):
        return {"sp": me, "tp": target}

    def peer_rank(step):
        return lax.rem(chip + step, chips) * 2 + parity

    def remote(src, dst, send, recv, device):
        return pltpu.make_async_remote_copy(
            src_ref=src,
            dst_ref=dst,
            send_sem=send,
            recv_sem=recv,
            device_id=device,
            device_id_type=MESH,
        )

    raw_loads = [
        pltpu.make_async_copy(source, raw.at[i], raw_sem.at[i])
        for i, source in enumerate((key_hbm, value_hbm, query_hbm))
    ]
    for copy in raw_loads:
        copy.start()
    pieces = down_send.shape[1]
    moved = units - ext
    per_core = moved // chunk
    weights = [
        pltpu.make_async_copy(out_hbm, out_w, weight_sem.at[0]),
        pltpu.make_async_copy(gate_hbm, gate, weight_sem.at[1]),
        pltpu.make_async_copy(up_hbm, up, weight_sem.at[2]),
        pltpu.make_async_copy(
            down_hbm.at[pl.ds(chip * 2 * units, 2 * units)], down_part.at[chip], weight_sem.at[3]
        ),
        pltpu.make_async_copy(residual_hbm, residual, weight_sem.at[4]),
    ]
    if ext:
        for step in range(1, chips):
            for core in range(2):
                start = (lax.rem(chip + step, chips) * 2 + core) * units + moved
                weights.append(
                    pltpu.make_async_copy(
                        down_hbm.at[pl.ds(start, ext)],
                        down_ext.at[step - 1, pl.ds(core * ext, ext)],
                        weight_sem.at[5 + (step - 1) * 2 + core],
                    )
                )

    barrier = pltpu.get_barrier_semaphore()
    for step in range(1, sp_size):
        pl.semaphore_signal(
            barrier, inc=1, device_id=at(lax.rem(me + step, sp_size)), device_id_type=MESH
        )
    for step in range(1, chips):
        pl.semaphore_signal(barrier, inc=1, device_id=beside(peer_rank(step)), device_id_type=MESH)
    pl.semaphore_signal(barrier, inc=1, device_id=beside(sibling), device_id_type=MESH)

    accum[...] = jnp.zeros(accum.shape, F32)
    peak[...] = jnp.full(peak.shape, NEG_FILL, F32)

    spare = -(-sp_size // 16) * 16
    names = lax.broadcasted_iota(jnp.int32, (spare, tokens), 0)
    named = [names == expert_ids[k : k + 1] for k in range(tops)]
    both = functools.reduce(jnp.logical_or, named).astype(F32).astype(BF16)
    before = (
        lax.broadcasted_iota(jnp.int32, (tokens, tokens), 0)
        < lax.broadcasted_iota(jnp.int32, (tokens, tokens), 1)
    ).astype(F32).astype(BF16)
    earlier = jnp.dot(both, before, preferred_element_type=F32)
    peak_logit = jnp.max(route_logit[...], axis=0, keepdims=True)
    shares = jnp.exp(route_logit[...] - peak_logit)
    shares = shares / jnp.sum(shares, axis=0, keepdims=True)
    for k in range(tops):
        order = jnp.sum(jnp.where(named[k], earlier, 0.0), axis=0, keepdims=True)
        expert = expert_ids[k : k + 1]
        apart = jnp.where(expert // reach == half_of, 0, reach)
        step_of = lax.rem(spot + reach - lax.rem(expert, reach), reach) + apart
        places[k : k + 1] = step_of * cap + order.astype(jnp.int32)

    for i in range(2):
        raw_loads[i].wait()
        blocks[me, :, i] = jnp.transpose(raw[i], (1, 0, 2))
    raw_loads[2].wait()
    low = lax.broadcasted_iota(jnp.int32, (heads, tokens, width), 2) < QK
    query = jnp.transpose(raw[2], (1, 0, 2)).astype(F32) * QK ** (-0.5)
    scaled[0] = jnp.where(low, query, 0.0).astype(BF16)
    scaled[1] = jnp.where(low, 0.0, query).astype(BF16)

    pl.semaphore_wait(barrier, sp_size - 1 + chips)

    def piece_row(piece):
        return piece // per_core * units + lax.rem(piece, per_core) * chunk

    def down_piece(step, piece):
        target = lax.rem(chip + step, chips)
        return remote(
            down_hbm.at[pl.ds(target * 2 * units + piece_row(piece), chunk)],
            down_part.at[chip, pl.ds(piece_row(piece), chunk)],
            down_send.at[step - 1, piece],
            down_recv.at[chip, piece],
            beside(target * 2 + parity),
        )

    def send_down(first, last):
        for step in range(1, chips):
            @pl.loop(first, last)
            def _(piece):
                down_piece(step, piece).start()

    pairs = sp_size // 2
    pair = me // 2
    side = lax.rem(me, 2)
    other = me + 1 - 2 * side

    def hand_on(block, send, back, target):
        return remote(
            blocks.at[block], blocks.at[block], send.at[back], kv_recv.at[block], at(target)
        )

    top = pairs - 1
    kept = heads // 2 if heads % 2 == 0 and pairs > 2 else heads

    def kept_part(block, send, back, target):
        part = blocks.at[block, pl.ds(0, kept)]
        return remote(part, part, send.at[back], kv_recv.at[block], at(target))

    def rest_part(block, target):
        part = blocks.at[block, pl.ds(kept, heads - kept)]
        return remote(part, part, rest_send, rest_recv, at(target))

    def attend(block, masked):
        if masked:
            key = block * tokens + lax.broadcasted_iota(jnp.int32, (tokens, tokens), 0)
            query = me * tokens + lax.broadcasted_iota(jnp.int32, (tokens, tokens), 1)
            visible = key // SPAN <= query // SPAN
        for head in range(heads):
            value = jnp.concatenate(
                [jnp.transpose(blocks[block, head, 1]), jnp.ones((16, tokens), BF16)], axis=0
            )
            for half in range(2):
                scores = lax.dot_general(
                    blocks[block, head, 0],
                    scaled[half, head],
                    (((1,), (1,)), ((), ())),
                    preferred_element_type=F32,
                )
                if masked:
                    scores = jnp.where(visible, scores, NEG_FILL)
                index = head * 2 + half
                old = peak[index]
                new = jnp.maximum(old, jnp.max(scores, axis=0, keepdims=True))
                exps = jnp.exp(scores - new)
                if masked:
                    exps = jnp.where(visible, exps, 0.0)
                peak[index] = new
                accum[index] = accum[index] * jnp.exp(old - new) + jnp.dot(
                    value, exps.astype(BF16), preferred_element_type=F32
                )

    plain_blocks = tokens % SPAN == 0

    @pl.loop(0, pair + 2)
    def _(back):
        @pl.when(back <= pair)
        def _():
            block = me - 2 * back

            @pl.when(back > 0)
            def _():
                hand_on(block, across_send, back, other).wait_recv()

            @pl.when(pair < pairs - 1)
            def _():
                hand_on(block, along_send, back, me + 2).start()

            cut = (pair == top) & (back == pair) & (kept < heads)

            @pl.when(((back > 0) | (side == 0)) & jnp.logical_not(cut))
            def _():
                hand_on(block, across_send, back, other).start()

            @pl.when(cut)
            def _():
                kept_part(block, across_send, back, other).start()

        @pl.when(back == 0)
        def _():
            send_down(0, pieces - 2)
            for copy in weights:
                copy.start()
            attend(me, True)

        second = other - 2 * (back - 1)
        use_second = (back >= 2) | ((back == 1) & (side == 1))

        @pl.loop(0, 2)
        def _(which):
            final = second == other - 2 * pair
            parted = (pair == top) & final & (kept < heads)

            @pl.when((which == 1) & use_second & jnp.logical_not(parted))
            def _():
                hand_on(second, across_send, 0, other).wait_recv()

            if kept < heads:
                @pl.when((which == 1) & use_second & parted)
                def _():
                    kept_part(second, across_send, 0, other).wait_recv()
                    rest_part(second, other).wait_recv()

                @pl.when((which == 1) & use_second & (pair == top - 1) & final)
                def _():
                    rest_part(second, me + 2).start()

            @pl.when(((which == 0) & (back > 0) & (back <= pair)) | ((which == 1) & use_second))
            def _():
                attend(jnp.where(which == 0, me - 2 * back, second), not plain_blocks)

    def piece(buffer, send, recv, owner, target, send_slot):
        return remote(
            buffer.at[owner],
            buffer.at[owner],
            send.at[send_slot],
            recv.at[owner],
            beside(target),
        )

    def spread(buffer, send, recv):
        for step in range(1, chips):
            target = peer_rank(step)
            piece(buffer, send, recv, rank, target, target).start()
        piece(buffer, send, recv, rank, sibling, sibling).start()

    def forward(buffer, send, recv, step):
        owner = peer_rank(step)
        onward = piece(buffer, send, recv, owner, sibling, owner + 1 - 2 * parity)
        onward.wait_recv()
        onward.start()

    def collect(buffer, send, recv):
        for step in range(chips):
            owner = peer_rank(step) + 1 - 2 * parity
            piece(buffer, send, recv, owner, sibling, sibling).wait_recv()

    def settle(buffer, send, recv):
        for step in range(1, chips):
            target = peer_rank(step)
            piece(buffer, send, recv, rank, target, target).wait_send()
            piece(buffer, send, recv, target, sibling, target + 1 - 2 * parity).wait_send()
        piece(buffer, send, recv, rank, sibling, sibling).wait_send()

    for head in range(heads):
        shrink = [
            1.0 / accum[index, width : width + 1] for index in (head * 2, head * 2 + 1)
        ]
        mixture = (
            accum[head * 2, :width] * shrink[0]
            - accum[head * 2 + 1, :width] * (diff_scale[head] * shrink[1])
        )
        scale_back = lax.rsqrt(jnp.mean(mixture * mixture, axis=0, keepdims=True) + NORM_EPS)
        heads_all[head, rank] = (
            jnp.transpose(mixture * scale_back) * head_gain[...] * HEAD_KEEP
        ).astype(BF16)
        spread(heads_all.at[head], att_send.at[head], att_recv.at[head])
    weights[0].wait()
    weights[4].wait()

    def project(owner):
        return jnp.dot(
            jnp.concatenate([heads_all[head, owner] for head in range(heads)], axis=1),
            out_w[pl.ds(pl.multiple_of(owner * heads * width, heads * width), heads * width)],
            preferred_element_type=F32,
        )

    sums = updated
    sums[...] = residual[...].astype(F32) + project(rank)
    for head in range(heads):
        for step in range(1, chips):
            forward(heads_all.at[head], att_send.at[head], att_recv.at[head], step)

    def from_sibling(step):
        owner = peer_rank(step) + 1 - 2 * parity
        for head in range(heads):
            piece(
                heads_all.at[head], att_send.at[head], att_recv.at[head], owner, sibling, sibling
            ).wait_recv()
        return project(owner)

    send_down(pieces - 2, pieces - 1)
    sums[...] += from_sibling(0)
    for step in range(1, chips):
        sums[...] += project(peer_rank(step))
    for step in range(1, chips):
        sums[...] += from_sibling(step)
    mixer[chip] = sums[...].astype(BF16)

    def mix_copy(step):
        target = lax.rem(chip + step, chips)
        return remote(
            mixer.at[chip],
            mixer.at[chip],
            mix_send.at[step - 1],
            mix_recv.at[chip],
            beside(target * 2 + parity),
        )

    for step in range(1, chips):
        mix_copy(step).start()

    def slots_of(first, count):
        slot = first + lax.broadcasted_iota(jnp.int32, (count, tokens), 0)
        return [slot == places[k : k + 1] for k in range(tops)]

    def chosen_rows(step, source):
        held = functools.reduce(jnp.logical_or, slots_of(step * cap, cap))
        return jnp.dot(
            held.astype(F32).astype(BF16), mixer[source], preferred_element_type=F32
        ).astype(BF16)

    def near_at(place):
        return at(half_of * reach + lax.rem(spot + reach + place, reach))

    def far_at(place):
        return at((1 - half_of) * reach + lax.rem(spot + reach + place, reach))

    def far_dispatch(place):
        return remote(
            far_out.at[place],
            far_rows.at[place // span, rank, pl.ds(lax.rem(place, span) * cap, cap)],
            far_send.at[place],
            far_recv.at[place],
            far_at(-place),
        )

    def near_dispatch(place, source):
        return remote(
            near_out.at[place, source],
            near_rows.at[source * 2 + parity, pl.ds(place * cap, cap)],
            near_send.at[place, source],
            near_recv.at[place, source],
            near_at(-place),
        )

    def send_near(source):
        near_rows[source * 2 + parity, pl.ds(0, cap), :] = chosen_rows(0, source)

        @pl.loop(1, reach)
        def _(place):
            near_out[place, source] = chosen_rows(place, source)
            near_dispatch(place, source).start()

    def send_far(first, last):
        @pl.loop(first, last)
        def _(place):
            far_out[place] = chosen_rows(reach + place, chip)
            far_dispatch(place).start()

    send_far(0, span)
    send_near(chip)
    send_far(span, span * ahead)
    for step in range(1, chips):
        source = lax.rem(chip + step, chips)
        remote(
            mixer.at[source],
            mixer.at[source],
            mix_send.at[step - 1],
            mix_recv.at[source],
            beside(sibling),
        ).wait_recv()
        send_near(source)
    send_far(span * ahead, reach)

    unit_tile = math.gcd(units, 256)
    column_tile = math.gcd(columns, 256)

    def spread_rows(group):
        for place in range(span):
            remote(
                far_out.at[0],
                far_rows.at[group, rank, pl.ds(place * cap, cap)],
                far_send.at[group * span + place],
                far_recv.at[group * span + place],
                beside(sibling),
            ).wait_recv()
        spread(far_rows.at[group], row_send.at[group], row_recv.at[group])

    def pair_copy(source):
        return remote(
            near_rows.at[source * 2 + parity],
            near_rows.at[source * 2 + parity],
            pair_send.at[source],
            pair_recv.at[source],
            beside(sibling),
        )

    def pair_rows():
        for step in range(chips):
            source = lax.rem(chip + step, chips)

            @pl.loop(1, reach)
            def _(place):
                remote(
                    near_out.at[0, 0],
                    near_rows.at[source * 2 + parity, pl.ds(place * cap, cap)],
                    near_send.at[place, source],
                    near_recv.at[place, source],
                    beside(sibling),
                ).wait_recv()

            pair_copy(source).start()

    def pair_wait():
        for step in range(chips):
            source = lax.rem(chip + step, chips)
            remote(
                near_rows.at[source * 2 + 1 - parity],
                near_rows.at[source * 2 + 1 - parity],
                pair_send.at[source],
                pair_recv.at[source],
                beside(sibling),
            ).wait_recv()

    def hidden_copy(hidden, index, core):
        return remote(
            hidden.at[core],
            hidden.at[core],
            hid_send.at[index],
            hid_recv.at[index],
            beside(sibling),
        )

    def ext_copy(hidden, extra, index, step):
        target = lax.rem(chip + step, chips)
        return remote(
            hidden.at[parity, :, pl.ds(moved, ext)],
            extra.at[chip, parity],
            ext_send.at[index, step - 1],
            ext_recv.at[index, chip, parity],
            beside(target * 2 + parity),
        )

    def ext_onward(extra, index, step, core):
        source = lax.rem(chip + step, chips)
        return remote(
            extra.at[source, core],
            extra.at[source, core],
            ext_over_send.at[index, step - 1],
            ext_recv.at[index, source, core],
            beside(sibling),
        )

    def ext_over(extra, index):
        if ext:
            for step in range(1, chips):
                onward = ext_onward(extra, index, step, parity)
                onward.wait_recv()
                onward.start()

    def ext_wait(extra, index):
        if ext:
            for step in range(1, chips):
                ext_onward(extra, index, step, 1 - parity).wait_recv()

    def send_ext(hidden, extra, index):
        if ext:
            for step in range(1, chips):
                ext_copy(hidden, extra, index, step).start()

    def run_up(table, hidden, extra, count, index, beat=None):
        square = 0.0
        for part in range(tp_size):
            value = table[part].astype(F32)
            square += jnp.sum(value * value, axis=-1, keepdims=True)
        scale_back = lax.rsqrt(square / (tp_size * feats) + NORM_EPS)
        for part in range(tp_size):
            depth = slice(part * feats, (part + 1) * feats)
            normed[:count, depth] = (
                table[part].astype(F32) * scale_back * norm_gain[:, depth]
            ).astype(BF16)

        @pl.loop(0, units // unit_tile)
        def _(tile):
            turned = lax.rem(tile + moved // unit_tile, units // unit_tile)
            cols = pl.ds(pl.multiple_of(turned * unit_tile, unit_tile), unit_tile)
            pre_gate = jnp.dot(normed[:count], gate[:, cols], preferred_element_type=F32)
            pre_up = jnp.dot(normed[:count], up[:, cols], preferred_element_type=F32)
            capped = jnp.minimum(pre_gate, CLAMP_LIMIT)
            linear = jnp.clip(pre_up, -CLAMP_LIMIT, CLAMP_LIMIT)
            value = capped * jax.nn.sigmoid(SWISH_ALPHA * capped) * (linear + 1.0)
            hidden[parity, :, cols] = value.astype(BF16)
            if index is not groups:
                @pl.when(tile == max(ext // unit_tile, 1) - 1)
                def _():
                    send_ext(hidden, extra, index)

            if beat is not None:
                beat(tile)

        hidden_copy(hidden, index, parity).start()

    def hand_over(group):
        for step in range(1, chips):
            forward(far_rows.at[group], row_send.at[group], row_recv.at[group], step)

    def far_up(group, beat=None):
        collect(far_rows.at[group], row_send.at[group], row_recv.at[group])
        run_up(far_rows.at[group], far_hidden.at[group], far_ext.at[group], rows, group, beat)

    def near_up(beat):
        pair_wait()
        run_up(near_rows, near_hidden, near_ext, near_count, groups, beat)

    def sum_copy(group, step):
        target = lax.rem(chip + step, chips)
        return remote(
            part_send.at[group, step - 1],
            part_recv.at[group, step - 1],
            sum_send.at[group, step - 1],
            sum_recv.at[group, step - 1],
            beside(target * 2 + parity),
        )

    def part_sum(hidden, block, cols):
        value = 0.0
        for core in range(2):
            value += jnp.dot(
                hidden[core, :, :moved],
                down_part[block, core * units : core * units + moved, cols],
                preferred_element_type=F32,
            )
        return value

    def own_part(hidden, extra, cols):
        value = 0.0
        for core in range(2):
            value += jnp.dot(
                hidden[core],
                down_part[chip, core * units : (core + 1) * units, cols],
                preferred_element_type=F32,
            )
        if ext:
            for step in range(1, chips):
                for core in range(2):
                    value += jnp.dot(
                        extra[lax.rem(chip + step, chips), core],
                        down_ext[step - 1, core * ext : (core + 1) * ext, cols],
                        preferred_element_type=F32,
                    )
        return value

    def column_loop(body):
        @pl.loop(0, columns // column_tile)
        def _(tile):
            body(pl.ds(pl.multiple_of(tile * column_tile, column_tile), column_tile))

    def down_ready():
        weights[3].wait()
        for step in range(1, chips):
            source = lax.rem(chip + step, chips)

            @pl.loop(0, pieces)
            def _(index):
                remote(
                    down_part.at[source, pl.ds(piece_row(index), chunk)],
                    down_part.at[source, pl.ds(piece_row(index), chunk)],
                    down_send.at[step - 1, index],
                    down_recv.at[source, index],
                    beside(sibling),
                ).wait_recv()

    def far_outward(group):
        hidden_copy(far_hidden.at[group], group, 1 - parity).wait_recv()
        for step in range(1, chips):
            def outward(cols):
                part_send[group, step - 1, :, cols] = part_sum(
                    far_hidden.at[group], lax.rem(chip + step, chips), cols
                ).astype(BF16)

            column_loop(outward)
            sum_copy(group, step).start()

    def far_inward(group):
        ext_wait(far_ext.at[group], group)

        def inward(cols):
            far_sum[group, :, cols] = own_part(far_hidden.at[group], far_ext.at[group], cols)

        column_loop(inward)

    def near_return(place, block):
        return remote(
            near_result.at[block, pl.ds(place * cap, cap)],
            near_back.at[block, pl.ds(place * cap, cap)],
            near_ret_send.at[place, block],
            near_ret_recv.at[place, block],
            near_at(place),
        )

    def near_down(steps):
        for step in steps:
            block = lax.rem(chip + step, chips)

            if step == chips:
                ext_wait(near_ext, groups)

            def store(cols):
                if step < chips:
                    value = part_sum(near_hidden, block, cols)
                else:
                    value = own_part(near_hidden, near_ext, cols)
                near_result[block, :, cols] = value.astype(BF16)

            column_loop(store)

            @pl.loop(1, reach)
            def _(place):
                near_return(place, block).start()

            near_back[block, pl.ds(0, cap), :] = near_result[block, pl.ds(0, cap), :]

    def give_back(place):
        return remote(
            far_result.at[place // span, pl.ds(lax.rem(place, span) * cap, cap)],
            far_back.at[place // span, pl.ds(lax.rem(place, span) * cap, cap)],
            far_ret_send.at[place],
            far_ret_recv.at[place],
            far_at(place),
        )

    def finish(group):
        value = far_sum[group]
        for step in range(1, chips):
            sum_copy(group, step).wait_recv()
            value += part_recv[group, step - 1].astype(F32)
        far_result[group] = value.astype(BF16)
        for place in range(span):
            give_back(group * span + place).start()

    def at_tiles(acts):
        def beat(tile):
            for number, act in acts:
                pl.when(tile == number)(act)

        return beat

    last_tile = units // unit_tile - 1
    first_part = list(range(ahead))
    second_part = list(range(ahead, groups))

    def second_out():
        for group in second_part:
            spread_rows(group)

    def first_ext():
        for group in first_part:
            ext_over(far_ext.at[group], group)

    def near_ext_out():
        send_ext(near_hidden, near_ext, groups)

    def first_done():
        for group in first_part:
            finish(group)

    weights[1].wait()
    weights[2].wait()
    for group in first_part:
        spread_rows(group)
        hand_over(group)
    send_down(pieces - 1, pieces)
    for group in first_part:
        far_up(group)
    pair_rows()
    down_ready()
    for group in first_part:
        far_outward(group)
    near_up(at_tiles([(0, second_out), (1, first_ext), (last_tile, near_ext_out)]))
    for copy in weights[5:]:
        copy.wait()
    for group in first_part:
        far_inward(group)
    first_done()
    hidden_copy(near_hidden, groups, 1 - parity).wait_recv()
    near_down(range(1, chips))
    for group in second_part:
        hand_over(group)
    for group in second_part:
        far_up(group)
    ext_over(near_ext, groups)
    for group in second_part:
        far_outward(group)
    near_down((chips,))
    for group in second_part:
        ext_over(far_ext.at[group], group)
    for group in second_part:
        far_inward(group)
    for group in second_part:
        finish(group)

    @pl.loop(0, pair + 1)
    def _(back):
        block = me - 2 * back

        @pl.when(pair < pairs - 1)
        def _():
            hand_on(block, along_send, back, me + 2).wait_send()

        cut = (pair == top) & (back == pair) & (kept < heads)

        @pl.when(((back > 0) | (side == 0)) & jnp.logical_not(cut))
        def _():
            hand_on(block, across_send, back, other).wait_send()

        @pl.when(cut)
        def _():
            kept_part(block, across_send, back, other).wait_send()

    if kept < heads:
        @pl.when(pair == top - 1)
        def _():
            rest_part(other - 2 * pair, me + 2).wait_send()

    for step in range(1, chips):
        @pl.loop(0, pieces)
        def _(index):
            down_piece(step, index).wait_send()

    for head in range(heads):
        settle(heads_all.at[head], att_send.at[head], att_recv.at[head])

    for step in range(1, chips):
        mix_copy(step).wait_send()

    @pl.loop(0, reach)
    def _(place):
        far_dispatch(place).wait_send()

    for source in range(chips):
        pair_copy(source).wait_send()

        @pl.loop(1, reach)
        def _(place):
            near_dispatch(place, source).wait_send()

    hidden_copy(near_hidden, groups, parity).wait_send()
    if ext:
        for step in range(1, chips):
            ext_copy(near_hidden, near_ext, groups, step).wait_send()
            ext_onward(near_ext, groups, step, parity).wait_send()

    @pl.loop(0, groups)
    def _(group):
        settle(far_rows.at[group], row_send.at[group], row_recv.at[group])
        hidden_copy(far_hidden.at[group], group, parity).wait_send()
        for step in range(1, chips):
            if ext:
                ext_copy(far_hidden.at[group], far_ext.at[group], group, step).wait_send()
                ext_onward(far_ext.at[group], group, step, parity).wait_send()
            sum_copy(group, step).wait_send()

    def routed_sum(first, count, table):
        portion = 0.0
        for k, held in enumerate(slots_of(first, count)):
            portion += jnp.where(held, shares[k : k + 1], 0.0)
        coarse = portion.astype(BF16)
        fine = (portion - coarse.astype(F32)).astype(BF16)
        value = 0.0
        for part in (coarse, fine):
            value += lax.dot_general(
                part, table, (((0,), (0,)), ((), ())), preferred_element_type=F32
            )
        return value

    def share_copy(step):
        target = lax.rem(chip + step, chips)
        return remote(
            share_send.at[step - 1],
            share_recv.at[step - 1],
            share_send_sem.at[step - 1],
            share_recv_sem.at[step - 1],
            beside(target * 2 + parity),
        )

    for step in range(1, chips + 1):
        block = lax.rem(chip + step, chips)

        @pl.loop(1, reach)
        def _(place):
            near_return(place, block).wait_recv()

        if step < chips:
            share_send[step - 1] = routed_sum(0, near_count, near_back[block]).astype(BF16)
            share_copy(step).start()
        else:
            sums[...] = mixer[chip].astype(F32) + routed_sum(0, near_count, near_back[chip])

    @pl.loop(0, groups)
    def _(group):
        for place in range(span):
            give_back(group * span + place).wait_recv()
        sums[...] += routed_sum(near_count + group * rows, rows, far_back[group])

    for step in range(1, chips):
        share_copy(step).wait_recv()
        sums[...] += share_recv[step - 1].astype(F32)

    for step in range(1, chips):
        share_copy(step).wait_send()

    @pl.loop(0, reach)
    def _(place):
        give_back(place).wait_send()

    for source in range(chips):
        @pl.loop(1, reach)
        def _(place):
            near_return(place, source).wait_send()


def local(
    residual,
    queries,
    key_rows,
    value_rows,
    diff_scale,
    head_gain,
    out_weight,
    norm_gain,
    gate_weight,
    up_weight,
    down_weight,
    expert_ids,
    route_logit,
):
    sp_size = lax.axis_size("sp")
    tp_size = lax.axis_size("tp")
    tokens, heads, width = value_rows.shape
    feats = residual.shape[1]
    tops = expert_ids.shape[1]
    cap = -(-(2 * tokens * tops // sp_size) // 16) * 16
    reach = sp_size // 2
    groups = math.gcd(reach, 2)
    rows = reach // groups * cap
    near_count = reach * cap
    units = gate_weight.shape[2]
    chips = tp_size // 2
    peers = max(chips - 1, 1)
    chunk = 2 * units // 16
    ext = units // 8 if units % 1024 == 0 else 0
    kept_ext = max(ext, 128)
    pieces = 2 * ((units - ext) // chunk)
    dma = pltpu.SemaphoreType.DMA
    vmem = pl.BlockSpec(memory_space=pltpu.VMEM)
    hbm = pl.BlockSpec(memory_space=pl.ANY)
    return pl.pallas_call(
        functools.partial(layer_kernel, sp_size, tp_size, groups, cap, ext, chunk),
        out_shape=jax.ShapeDtypeStruct((tokens, feats), F32),
        in_specs=[
            hbm,
            hbm,
            hbm,
            hbm,
            pl.BlockSpec(memory_space=pltpu.SMEM),
            vmem,
            hbm,
            vmem,
            hbm,
            hbm,
            hbm,
            vmem,
            vmem,
        ],
        out_specs=vmem,
        scratch_shapes=[
            pltpu.VMEM((tokens, feats), BF16),
            pltpu.VMEM((3, tokens, heads, width), BF16),
            pltpu.VMEM((2, heads, tokens, width), BF16),
            pltpu.VMEM((sp_size, heads, 2, tokens, width), BF16),
            pltpu.VMEM((heads * 2, 1, tokens), F32),
            pltpu.VMEM((heads * 2, width + 16, tokens), F32),
            pltpu.VMEM((heads, tp_size, tokens, width), BF16),
            pltpu.VMEM(out_weight.shape, BF16),
            pltpu.VMEM((chips, tokens, feats), BF16),
            pltpu.VMEM((tops, tokens), jnp.int32),
            pltpu.VMEM((reach, chips, cap, feats), BF16),
            pltpu.VMEM((reach, cap, feats), BF16),
            pltpu.VMEM((tp_size, near_count, feats), BF16),
            pltpu.VMEM((groups, tp_size, rows, feats), BF16),
            pltpu.VMEM((near_count, tp_size * feats), BF16),
            pltpu.VMEM((2, near_count, units), BF16),
            pltpu.VMEM((groups, 2, rows, units), BF16),
            pltpu.VMEM((groups, chips, 2, rows, kept_ext), BF16),
            pltpu.VMEM((chips, 2, near_count, kept_ext), BF16),
            pltpu.VMEM((chips, 2 * units, feats), BF16),
            pltpu.VMEM((peers, 2 * kept_ext, feats), BF16),
            pltpu.VMEM((tokens, feats), F32),
            pltpu.VMEM((groups, rows, feats), F32),
            pltpu.VMEM((groups, peers, rows, feats), BF16),
            pltpu.VMEM((groups, peers, rows, feats), BF16),
            pltpu.VMEM((chips, near_count, feats), BF16),
            pltpu.VMEM((groups, rows, feats), BF16),
            pltpu.VMEM((chips, near_count, feats), BF16),
            pltpu.VMEM((groups, rows, feats), BF16),
            pltpu.VMEM((peers, tokens, feats), BF16),
            pltpu.VMEM((peers, tokens, feats), BF16),
            pltpu.VMEM(gate_weight.shape[1:], BF16),
            pltpu.VMEM(up_weight.shape[1:], BF16),
            dma((5 + 2 * peers,)),
            dma((3,)),
            dma((sp_size,)),
            dma((sp_size,)),
            dma((sp_size,)),
            dma(()),
            dma(()),
            dma((peers, pieces)),
            dma((chips, pieces)),
            dma((heads, tp_size)),
            dma((heads, tp_size)),
            dma((peers,)),
            dma((chips,)),
            dma((reach, chips)),
            dma((reach, chips)),
            dma((reach,)),
            dma((reach,)),
            dma((chips,)),
            dma((chips,)),
            dma((groups, tp_size)),
            dma((groups, tp_size)),
            dma((groups + 1,)),
            dma((groups + 1,)),
            dma((groups + 1, peers)),
            dma((groups + 1, chips, 2)),
            dma((groups + 1, peers)),
            dma((groups, peers)),
            dma((groups, peers)),
            dma((reach, chips)),
            dma((reach, chips)),
            dma((reach,)),
            dma((reach,)),
            dma((peers,)),
            dma((peers,)),
        ],
        compiler_params=pltpu.CompilerParams(
            collective_id=0, has_side_effects=True, vmem_limit_bytes=56 * 1024 * 1024
        ),
    )(
        residual,
        queries,
        key_rows,
        value_rows,
        diff_scale,
        head_gain[None],
        out_weight,
        norm_gain[None],
        gate_weight[0],
        up_weight[0],
        down_weight[0],
        expert_ids.T,
        route_logit.T,
    ).astype(BF16)


def solution(mesh):
    return jax.shard_map(
        local,
        mesh=mesh,
        in_specs=(
            P("sp", "tp"),
            P("sp", "tp", None),
            P("sp", "tp", None),
            P("sp", "tp", None),
            P("tp"),
            P(),
            P(None, "tp"),
            P(),
            P("sp", None, "tp"),
            P("sp", None, "tp"),
            P("sp", None, "tp"),
            P("sp", None),
            P("sp", None),
        ),
        out_specs=P("sp", "tp"),
        check_vma=False,
    )
```

```python
import functools
import math

import jax
import jax.numpy as jnp
from jax import lax
from jax.experimental import pallas as pl
from jax.experimental.pallas import tpu as pltpu
from jax.sharding import PartitionSpec as P

D = 2048
QK = 64
SPAN = 64


NORM_EPS = 1e-05
CLAMP_LIMIT = 7.0
SWISH_ALPHA = 1.702
HEAD_KEEP = 0.8
NEG_FILL = -1e30
MESH = pl.DeviceIdType.MESH
F32 = jnp.float32
BF16 = jnp.bfloat16


def layer_kernel(
    sp_size,
    tp_size,
    groups,
    cap,
    ext,
    chunk,
    residual_hbm,
    query_hbm,
    key_hbm,
    value_hbm,
    diff_scale,
    head_gain,
    out_hbm,
    norm_gain,
    gate_hbm,
    up_hbm,
    down_hbm,
    expert_ids,
    route_logit,
    updated,
    residual,
    raw,
    scaled,
    blocks,
    peak,
    accum,
    heads_all,
    out_w,
    mixer,
    places,
    near_out,
    far_out,
    near_rows,
    far_rows,
    normed,
    near_hidden,
    far_hidden,
    far_ext,
    near_ext,
    down_part,
    down_ext,
    own_sum,
    far_sum,
    part_send,
    part_recv,
    near_result,
    far_result,
    near_back,
    far_back,
    share_send,
    share_recv,
    gate,
    up,
    weight_sem,
    raw_sem,
    along_send,
    across_send,
    kv_recv,
    rest_send,
    rest_recv,
    down_send,
    down_recv,
    att_send,
    att_recv,
    mix_send,
    mix_recv,
    near_send,
    near_recv,
    far_send,
    far_recv,
    pair_send,
    pair_recv,
    row_send,
    row_recv,
    hid_send,
    hid_recv,
    ext_send,
    ext_recv,
    ext_over_send,
    sum_send,
    sum_recv,
    near_ret_send,
    near_ret_recv,
    far_ret_send,
    far_ret_recv,
    share_send_sem,
    share_recv_sem,
):
    me = lax.axis_index("sp")
    rank = lax.axis_index("tp")
    parity = lax.rem(rank, 2)
    sibling = rank + 1 - 2 * parity
    chips = tp_size // 2
    chip = rank // 2
    reach = sp_size // 2
    half_of = me // reach
    spot = lax.rem(me, reach)
    span = reach // groups
    ahead = (groups + 1) // 2
    rows = span * cap
    near_count = reach * cap
    tokens, heads, width = query_hbm.shape
    feats = residual.shape[1]
    units = gate.shape[1]
    columns = feats
    tops = expert_ids.shape[0]

    def at(index):
        return {"sp": index, "tp": rank}

    def beside(target):
        return {"sp": me, "tp": target}

    def peer_rank(step):
        return lax.rem(chip + step, chips) * 2 + parity

    def remote(src, dst, send, recv, device):
        return pltpu.make_async_remote_copy(
            src_ref=src,
            dst_ref=dst,
            send_sem=send,
            recv_sem=recv,
            device_id=device,
            device_id_type=MESH,
        )

    raw_loads = [
        pltpu.make_async_copy(source, raw.at[i], raw_sem.at[i])
        for i, source in enumerate((key_hbm, value_hbm, query_hbm))
    ]
    for copy in raw_loads:
        copy.start()
    pieces = down_send.shape[1]
    moved = units - ext
    per_core = moved // chunk
    weights = [
        pltpu.make_async_copy(out_hbm, out_w, weight_sem.at[0]),
        pltpu.make_async_copy(gate_hbm, gate, weight_sem.at[1]),
        pltpu.make_async_copy(up_hbm, up, weight_sem.at[2]),
        pltpu.make_async_copy(
            down_hbm.at[pl.ds(chip * 2 * units, 2 * units)], down_part.at[chip], weight_sem.at[3]
        ),
        pltpu.make_async_copy(residual_hbm, residual, weight_sem.at[4]),
    ]
    if ext:
        for step in range(1, chips):
            for core in range(2):
                start = (lax.rem(chip + step, chips) * 2 + core) * units + moved
                weights.append(
                    pltpu.make_async_copy(
                        down_hbm.at[pl.ds(start, ext)],
                        down_ext.at[step - 1, pl.ds(core * ext, ext)],
                        weight_sem.at[5 + (step - 1) * 2 + core],
                    )
                )

    barrier = pltpu.get_barrier_semaphore()
    for step in range(1, sp_size):
        pl.semaphore_signal(
            barrier, inc=1, device_id=at(lax.rem(me + step, sp_size)), device_id_type=MESH
        )
    for step in range(1, chips):
        pl.semaphore_signal(barrier, inc=1, device_id=beside(peer_rank(step)), device_id_type=MESH)
    pl.semaphore_signal(barrier, inc=1, device_id=beside(sibling), device_id_type=MESH)

    accum[...] = jnp.zeros(accum.shape, F32)
    peak[...] = jnp.full(peak.shape, NEG_FILL, F32)

    spare = -(-sp_size // 16) * 16
    names = lax.broadcasted_iota(jnp.int32, (spare, tokens), 0)
    named = [names == expert_ids[k : k + 1] for k in range(tops)]
    both = functools.reduce(jnp.logical_or, named).astype(F32).astype(BF16)
    before = (
        lax.broadcasted_iota(jnp.int32, (tokens, tokens), 0)
        < lax.broadcasted_iota(jnp.int32, (tokens, tokens), 1)
    ).astype(F32).astype(BF16)
    earlier = jnp.dot(both, before, preferred_element_type=F32)
    peak_logit = jnp.max(route_logit[...], axis=0, keepdims=True)
    shares = jnp.exp(route_logit[...] - peak_logit)
    shares = shares / jnp.sum(shares, axis=0, keepdims=True)
    for k in range(tops):
        order = jnp.sum(jnp.where(named[k], earlier, 0.0), axis=0, keepdims=True)
        expert = expert_ids[k : k + 1]
        apart = jnp.where(expert // reach == half_of, 0, reach)
        step_of = lax.rem(spot + reach - lax.rem(expert, reach), reach) + apart
        places[k : k + 1] = step_of * cap + order.astype(jnp.int32)

    for i in range(2):
        raw_loads[i].wait()
        blocks[me, :, i] = jnp.transpose(raw[i], (1, 0, 2))
    raw_loads[2].wait()
    low = lax.broadcasted_iota(jnp.int32, (heads, tokens, width), 2) < QK
    query = jnp.transpose(raw[2], (1, 0, 2)).astype(F32) * QK ** (-0.5)
    scaled[0] = jnp.where(low, query, 0.0).astype(BF16)
    scaled[1] = jnp.where(low, 0.0, query).astype(BF16)

    pl.semaphore_wait(barrier, sp_size - 1 + chips)

    def piece_row(piece):
        return piece // per_core * units + lax.rem(piece, per_core) * chunk

    def down_piece(step, piece):
        target = lax.rem(chip + step, chips)
        return remote(
            down_hbm.at[pl.ds(target * 2 * units + piece_row(piece), chunk)],
            down_part.at[chip, pl.ds(piece_row(piece), chunk)],
            down_send.at[step - 1, piece],
            down_recv.at[chip, piece],
            beside(target * 2 + parity),
        )

    def send_down(first, last):
        for step in range(1, chips):
            @pl.loop(first, last)
            def _(piece):
                down_piece(step, piece).start()

    pairs = sp_size // 2
    pair = me // 2
    side = lax.rem(me, 2)
    other = me + 1 - 2 * side

    def hand_on(block, send, back, target):
        return remote(
            blocks.at[block], blocks.at[block], send.at[back], kv_recv.at[block], at(target)
        )

    top = pairs - 1
    kept = heads // 2 if heads % 2 == 0 and pairs > 2 else heads

    def kept_part(block, send, back, target):
        part = blocks.at[block, pl.ds(0, kept)]
        return remote(part, part, send.at[back], kv_recv.at[block], at(target))

    def rest_part(block, target):
        part = blocks.at[block, pl.ds(kept, heads - kept)]
        return remote(part, part, rest_send, rest_recv, at(target))

    def attend(block, masked):
        if masked:
            key = block * tokens + lax.broadcasted_iota(jnp.int32, (tokens, tokens), 0)
            query = me * tokens + lax.broadcasted_iota(jnp.int32, (tokens, tokens), 1)
            visible = key // SPAN <= query // SPAN
        for head in range(heads):
            value = jnp.concatenate(
                [jnp.transpose(blocks[block, head, 1]), jnp.ones((16, tokens), BF16)], axis=0
            )
            for half in range(2):
                scores = lax.dot_general(
                    blocks[block, head, 0],
                    scaled[half, head],
                    (((1,), (1,)), ((), ())),
                    preferred_element_type=F32,
                )
                if masked:
                    scores = jnp.where(visible, scores, NEG_FILL)
                index = head * 2 + half
                old = peak[index]
                new = jnp.maximum(old, jnp.max(scores, axis=0, keepdims=True))
                exps = jnp.exp(scores - new)
                if masked:
                    exps = jnp.where(visible, exps, 0.0)
                peak[index] = new
                accum[index] = accum[index] * jnp.exp(old - new) + jnp.dot(
                    value, exps.astype(BF16), preferred_element_type=F32
                )

    plain_blocks = tokens % SPAN == 0

    @pl.loop(0, pair + 2)
    def _(back):
        @pl.when(back <= pair)
        def _():
            block = me - 2 * back

            @pl.when(back > 0)
            def _():
                hand_on(block, across_send, back, other).wait_recv()

            @pl.when(pair < pairs - 1)
            def _():
                hand_on(block, along_send, back, me + 2).start()

            cut = (pair == top) & (back == pair) & (kept < heads)

            @pl.when(((back > 0) | (side == 0)) & jnp.logical_not(cut))
            def _():
                hand_on(block, across_send, back, other).start()

            @pl.when(cut)
            def _():
                kept_part(block, across_send, back, other).start()

        @pl.when(back == 0)
        def _():
            send_down(0, pieces - 2)
            for copy in weights:
                copy.start()
            attend(me, True)

        second = other - 2 * (back - 1)
        use_second = (back >= 2) | ((back == 1) & (side == 1))

        @pl.loop(0, 2)
        def _(which):
            final = second == other - 2 * pair
            parted = (pair == top) & final & (kept < heads)

            @pl.when((which == 1) & use_second & jnp.logical_not(parted))
            def _():
                hand_on(second, across_send, 0, other).wait_recv()

            if kept < heads:
                @pl.when((which == 1) & use_second & parted)
                def _():
                    kept_part(second, across_send, 0, other).wait_recv()
                    rest_part(second, other).wait_recv()

                @pl.when((which == 1) & use_second & (pair == top - 1) & final)
                def _():
                    rest_part(second, me + 2).start()

            @pl.when(((which == 0) & (back > 0) & (back <= pair)) | ((which == 1) & use_second))
            def _():
                attend(jnp.where(which == 0, me - 2 * back, second), not plain_blocks)

    def piece(buffer, send, recv, owner, target, send_slot):
        return remote(
            buffer.at[owner],
            buffer.at[owner],
            send.at[send_slot],
            recv.at[owner],
            beside(target),
        )

    def spread(buffer, send, recv):
        for step in range(1, chips):
            target = peer_rank(step)
            piece(buffer, send, recv, rank, target, target).start()
        piece(buffer, send, recv, rank, sibling, sibling).start()

    def forward(buffer, send, recv, step):
        owner = peer_rank(step)
        onward = piece(buffer, send, recv, owner, sibling, owner + 1 - 2 * parity)
        onward.wait_recv()
        onward.start()

    def collect(buffer, send, recv):
        for step in range(chips):
            owner = peer_rank(step) + 1 - 2 * parity
            piece(buffer, send, recv, owner, sibling, sibling).wait_recv()

    def settle(buffer, send, recv):
        for step in range(1, chips):
            target = peer_rank(step)
            piece(buffer, send, recv, rank, target, target).wait_send()
            piece(buffer, send, recv, target, sibling, target + 1 - 2 * parity).wait_send()
        piece(buffer, send, recv, rank, sibling, sibling).wait_send()

    for head in range(heads):
        shrink = [
            1.0 / accum[index, width : width + 1] for index in (head * 2, head * 2 + 1)
        ]
        mixture = (
            accum[head * 2, :width] * shrink[0]
            - accum[head * 2 + 1, :width] * (diff_scale[head] * shrink[1])
        )
        scale_back = lax.rsqrt(jnp.mean(mixture * mixture, axis=0, keepdims=True) + NORM_EPS)
        heads_all[head, rank] = (
            jnp.transpose(mixture * scale_back) * head_gain[...] * HEAD_KEEP
        ).astype(BF16)
        spread(heads_all.at[head], att_send.at[head], att_recv.at[head])
    weights[0].wait()
    weights[4].wait()

    def project(owner):
        return jnp.dot(
            jnp.concatenate([heads_all[head, owner] for head in range(heads)], axis=1),
            out_w[pl.ds(pl.multiple_of(owner * heads * width, heads * width), heads * width)],
            preferred_element_type=F32,
        )

    sums = updated
    sums[...] = residual[...].astype(F32) + project(rank)
    for head in range(heads):
        for step in range(1, chips):
            forward(heads_all.at[head], att_send.at[head], att_recv.at[head], step)

    def from_sibling(step):
        owner = peer_rank(step) + 1 - 2 * parity
        for head in range(heads):
            piece(
                heads_all.at[head], att_send.at[head], att_recv.at[head], owner, sibling, sibling
            ).wait_recv()
        return project(owner)

    send_down(pieces - 2, pieces - 1)
    sums[...] += from_sibling(0)
    for step in range(1, chips):
        sums[...] += project(peer_rank(step))
    for step in range(1, chips):
        sums[...] += from_sibling(step)
    mixer[chip] = sums[...].astype(BF16)

    def mix_copy(step):
        target = lax.rem(chip + step, chips)
        return remote(
            mixer.at[chip],
            mixer.at[chip],
            mix_send.at[step - 1],
            mix_recv.at[chip],
            beside(target * 2 + parity),
        )

    for step in range(1, chips):
        mix_copy(step).start()

    def slots_of(first, count):
        slot = first + lax.broadcasted_iota(jnp.int32, (count, tokens), 0)
        return [slot == places[k : k + 1] for k in range(tops)]

    def chosen_rows(step, source):
        held = functools.reduce(jnp.logical_or, slots_of(step * cap, cap))
        return jnp.dot(
            held.astype(F32).astype(BF16), mixer[source], preferred_element_type=F32
        ).astype(BF16)

    def near_at(place):
        return at(half_of * reach + lax.rem(spot + reach + place, reach))

    def far_at(place):
        return at((1 - half_of) * reach + lax.rem(spot + reach + place, reach))

    def far_dispatch(place):
        return remote(
            far_out.at[place],
            far_rows.at[place // span, rank, pl.ds(lax.rem(place, span) * cap, cap)],
            far_send.at[place],
            far_recv.at[place],
            far_at(-place),
        )

    def near_dispatch(place, source):
        return remote(
            near_out.at[place, source],
            near_rows.at[source * 2 + parity, pl.ds(place * cap, cap)],
            near_send.at[place, source],
            near_recv.at[place, source],
            near_at(-place),
        )

    def send_near(source):
        near_rows[source * 2 + parity, pl.ds(0, cap), :] = chosen_rows(0, source)

        @pl.loop(1, reach)
        def _(place):
            near_out[place, source] = chosen_rows(place, source)
            near_dispatch(place, source).start()

    def send_far(first, last):
        @pl.loop(first, last)
        def _(place):
            far_out[place] = chosen_rows(reach + place, chip)
            far_dispatch(place).start()

    send_far(0, span)
    send_near(chip)
    send_far(span, span * ahead)
    for step in range(1, chips):
        source = lax.rem(chip + step, chips)
        remote(
            mixer.at[source],
            mixer.at[source],
            mix_send.at[step - 1],
            mix_recv.at[source],
            beside(sibling),
        ).wait_recv()
        send_near(source)
    send_far(span * ahead, reach)

    unit_tile = math.gcd(units, 256)
    column_tile = math.gcd(columns, 256)

    def row_part(group, place):
        return (
            far_rows.at[group, :, pl.ds(place * cap, cap)],
            row_send.at[group, place],
            row_recv.at[group, place],
        )

    def spread_rows(group):
        @pl.loop(0, span)
        def _(place):
            remote(
                far_out.at[0],
                far_rows.at[group, rank, pl.ds(place * cap, cap)],
                far_send.at[group * span + place],
                far_recv.at[group * span + place],
                beside(sibling),
            ).wait_recv()
            spread(*row_part(group, place))

    def pair_copy(source):
        return remote(
            near_rows.at[source * 2 + parity],
            near_rows.at[source * 2 + parity],
            pair_send.at[source],
            pair_recv.at[source],
            beside(sibling),
        )

    def pair_rows():
        for step in range(chips):
            source = lax.rem(chip + step, chips)

            @pl.loop(1, reach)
            def _(place):
                remote(
                    near_out.at[0, 0],
                    near_rows.at[source * 2 + parity, pl.ds(place * cap, cap)],
                    near_send.at[place, source],
                    near_recv.at[place, source],
                    beside(sibling),
                ).wait_recv()

            pair_copy(source).start()

    def pair_wait():
        for step in range(chips):
            source = lax.rem(chip + step, chips)
            remote(
                near_rows.at[source * 2 + 1 - parity],
                near_rows.at[source * 2 + 1 - parity],
                pair_send.at[source],
                pair_recv.at[source],
                beside(sibling),
            ).wait_recv()

    def hidden_copy(hidden, index, core):
        return remote(
            hidden.at[core],
            hidden.at[core],
            hid_send.at[index],
            hid_recv.at[index],
            beside(sibling),
        )

    def ext_copy(hidden, extra, index, step):
        target = lax.rem(chip + step, chips)
        return remote(
            hidden.at[parity, :, pl.ds(moved, ext)],
            extra.at[chip, parity],
            ext_send.at[index, step - 1],
            ext_recv.at[index, chip, parity],
            beside(target * 2 + parity),
        )

    def ext_onward(extra, index, step, core):
        source = lax.rem(chip + step, chips)
        return remote(
            extra.at[source, core],
            extra.at[source, core],
            ext_over_send.at[index, step - 1],
            ext_recv.at[index, source, core],
            beside(sibling),
        )

    def ext_over(extra, index):
        if ext:
            for step in range(1, chips):
                onward = ext_onward(extra, index, step, parity)
                onward.wait_recv()
                onward.start()

    def ext_wait(extra, index):
        if ext:
            for step in range(1, chips):
                ext_onward(extra, index, step, 1 - parity).wait_recv()

    def send_ext(hidden, extra, index):
        if ext:
            for step in range(1, chips):
                ext_copy(hidden, extra, index, step).start()

    def run_up(table, hidden, extra, count, index, beat=None):
        square = 0.0
        for part in range(tp_size):
            value = table[part].astype(F32)
            square += jnp.sum(value * value, axis=-1, keepdims=True)
        scale_back = lax.rsqrt(square / (tp_size * feats) + NORM_EPS)
        for part in range(tp_size):
            depth = slice(part * feats, (part + 1) * feats)
            normed[:count, depth] = (
                table[part].astype(F32) * scale_back * norm_gain[:, depth]
            ).astype(BF16)

        @pl.loop(0, units // unit_tile)
        def _(tile):
            turned = lax.rem(tile + moved // unit_tile, units // unit_tile)
            cols = pl.ds(pl.multiple_of(turned * unit_tile, unit_tile), unit_tile)
            pre_gate = jnp.dot(normed[:count], gate[:, cols], preferred_element_type=F32)
            pre_up = jnp.dot(normed[:count], up[:, cols], preferred_element_type=F32)
            capped = jnp.minimum(pre_gate, CLAMP_LIMIT)
            linear = jnp.clip(pre_up, -CLAMP_LIMIT, CLAMP_LIMIT)
            value = capped * jax.nn.sigmoid(SWISH_ALPHA * capped) * (linear + 1.0)
            hidden[parity, :, cols] = value.astype(BF16)
            if index is not groups:
                @pl.when(tile == max(ext // unit_tile, 1) - 1)
                def _():
                    send_ext(hidden, extra, index)

            if beat is not None:
                beat(tile)

        hidden_copy(hidden, index, parity).start()

    def hand_over(group):
        @pl.loop(0, span)
        def _(place):
            for step in range(1, chips):
                forward(*row_part(group, place), step)

    def far_up(group, beat=None):
        @pl.loop(0, span)
        def _(place):
            collect(*row_part(group, place))

        run_up(far_rows.at[group], far_hidden.at[group], far_ext.at[group], rows, group, beat)

    def near_up(beat):
        pair_wait()
        run_up(near_rows, near_hidden, near_ext, near_count, groups, beat)

    def sum_copy(group, step):
        target = lax.rem(chip + step, chips)
        return remote(
            part_send.at[group, step - 1],
            part_recv.at[group, step - 1],
            sum_send.at[group, step - 1],
            sum_recv.at[group, step - 1],
            beside(target * 2 + parity),
        )

    def part_sum(hidden, block, cols):
        value = 0.0
        for core in range(2):
            value += jnp.dot(
                hidden[core, :, :moved],
                down_part[block, core * units : core * units + moved, cols],
                preferred_element_type=F32,
            )
        return value

    def own_part(hidden, extra, cols):
        value = 0.0
        for core in range(2):
            value += jnp.dot(
                hidden[core],
                down_part[chip, core * units : (core + 1) * units, cols],
                preferred_element_type=F32,
            )
        if ext:
            for step in range(1, chips):
                for core in range(2):
                    value += jnp.dot(
                        extra[lax.rem(chip + step, chips), core],
                        down_ext[step - 1, core * ext : (core + 1) * ext, cols],
                        preferred_element_type=F32,
                    )
        return value

    def column_loop(body):
        @pl.loop(0, columns // column_tile)
        def _(tile):
            body(pl.ds(pl.multiple_of(tile * column_tile, column_tile), column_tile))

    def down_ready():
        weights[3].wait()
        for step in range(1, chips):
            source = lax.rem(chip + step, chips)

            @pl.loop(0, pieces)
            def _(index):
                remote(
                    down_part.at[source, pl.ds(piece_row(index), chunk)],
                    down_part.at[source, pl.ds(piece_row(index), chunk)],
                    down_send.at[step - 1, index],
                    down_recv.at[source, index],
                    beside(sibling),
                ).wait_recv()

    def far_outward(group):
        hidden_copy(far_hidden.at[group], group, 1 - parity).wait_recv()
        for step in range(1, chips):
            def outward(cols):
                part_send[group, step - 1, :, cols] = part_sum(
                    far_hidden.at[group], lax.rem(chip + step, chips), cols
                ).astype(BF16)

            column_loop(outward)
            sum_copy(group, step).start()

    def far_inward(group):
        ext_wait(far_ext.at[group], group)

        def inward(cols):
            far_sum[group, :, cols] = own_part(far_hidden.at[group], far_ext.at[group], cols)

        column_loop(inward)

    def near_return(place, block):
        return remote(
            near_result.at[block, pl.ds(place * cap, cap)],
            near_back.at[block, pl.ds(place * cap, cap)],
            near_ret_send.at[place, block],
            near_ret_recv.at[place, block],
            near_at(place),
        )

    def near_down(steps):
        for step in steps:
            block = lax.rem(chip + step, chips)

            if step == chips:
                ext_wait(near_ext, groups)

            def store(cols):
                if step < chips:
                    value = part_sum(near_hidden, block, cols)
                else:
                    value = own_part(near_hidden, near_ext, cols)
                near_result[block, :, cols] = value.astype(BF16)

            column_loop(store)

            @pl.loop(1, reach)
            def _(place):
                near_return(place, block).start()

            near_back[block, pl.ds(0, cap), :] = near_result[block, pl.ds(0, cap), :]

    def give_back(place):
        return remote(
            far_result.at[place // span, pl.ds(lax.rem(place, span) * cap, cap)],
            far_back.at[place // span, pl.ds(lax.rem(place, span) * cap, cap)],
            far_ret_send.at[place],
            far_ret_recv.at[place],
            far_at(place),
        )

    def finish(group):
        value = far_sum[group]
        for step in range(1, chips):
            sum_copy(group, step).wait_recv()
            value += part_recv[group, step - 1].astype(F32)
        far_result[group] = value.astype(BF16)
        for place in range(span):
            give_back(group * span + place).start()

    def at_tiles(acts):
        def beat(tile):
            for number, act in acts:
                pl.when(tile == number)(act)

        return beat

    last_tile = units // unit_tile - 1
    first_part = list(range(ahead))
    second_part = list(range(ahead, groups))

    def second_out():
        for group in second_part:
            spread_rows(group)

    def first_ext():
        for group in first_part:
            ext_over(far_ext.at[group], group)

    def near_ext_out():
        send_ext(near_hidden, near_ext, groups)

    def first_done():
        for group in first_part:
            finish(group)

    weights[1].wait()
    weights[2].wait()
    for group in first_part:
        spread_rows(group)
        hand_over(group)
    send_down(pieces - 1, pieces)
    for group in first_part:
        far_up(group)
    pair_rows()
    down_ready()
    for group in first_part:
        far_outward(group)
    near_up(at_tiles([(0, second_out), (1, first_ext), (last_tile, near_ext_out)]))
    for copy in weights[5:]:
        copy.wait()
    for group in first_part:
        far_inward(group)
    first_done()
    hidden_copy(near_hidden, groups, 1 - parity).wait_recv()
    near_down(range(1, chips))
    for group in second_part:
        hand_over(group)
    for group in second_part:
        far_up(group)
    ext_over(near_ext, groups)
    for group in second_part:
        far_outward(group)
    near_down((chips,))
    for group in second_part:
        ext_over(far_ext.at[group], group)
    for group in second_part:
        far_inward(group)
    for group in second_part:
        finish(group)

    @pl.loop(0, pair + 1)
    def _(back):
        block = me - 2 * back

        @pl.when(pair < pairs - 1)
        def _():
            hand_on(block, along_send, back, me + 2).wait_send()

        cut = (pair == top) & (back == pair) & (kept < heads)

        @pl.when(((back > 0) | (side == 0)) & jnp.logical_not(cut))
        def _():
            hand_on(block, across_send, back, other).wait_send()

        @pl.when(cut)
        def _():
            kept_part(block, across_send, back, other).wait_send()

    if kept < heads:
        @pl.when(pair == top - 1)
        def _():
            rest_part(other - 2 * pair, me + 2).wait_send()

    for step in range(1, chips):
        @pl.loop(0, pieces)
        def _(index):
            down_piece(step, index).wait_send()

    for head in range(heads):
        settle(heads_all.at[head], att_send.at[head], att_recv.at[head])

    for step in range(1, chips):
        mix_copy(step).wait_send()

    @pl.loop(0, reach)
    def _(place):
        far_dispatch(place).wait_send()

    for source in range(chips):
        pair_copy(source).wait_send()

        @pl.loop(1, reach)
        def _(place):
            near_dispatch(place, source).wait_send()

    hidden_copy(near_hidden, groups, parity).wait_send()
    if ext:
        for step in range(1, chips):
            ext_copy(near_hidden, near_ext, groups, step).wait_send()
            ext_onward(near_ext, groups, step, parity).wait_send()

    @pl.loop(0, groups)
    def _(group):
        @pl.loop(0, span)
        def _(place):
            settle(*row_part(group, place))

        hidden_copy(far_hidden.at[group], group, parity).wait_send()
        for step in range(1, chips):
            if ext:
                ext_copy(far_hidden.at[group], far_ext.at[group], group, step).wait_send()
                ext_onward(far_ext.at[group], group, step, parity).wait_send()
            sum_copy(group, step).wait_send()

    def routed_sum(first, count, table):
        portion = 0.0
        for k, held in enumerate(slots_of(first, count)):
            portion += jnp.where(held, shares[k : k + 1], 0.0)
        coarse = portion.astype(BF16)
        fine = (portion - coarse.astype(F32)).astype(BF16)
        value = 0.0
        for part in (coarse, fine):
            value += lax.dot_general(
                part, table, (((0,), (0,)), ((), ())), preferred_element_type=F32
            )
        return value

    def share_copy(step):
        target = lax.rem(chip + step, chips)
        return remote(
            share_send.at[step - 1],
            share_recv.at[step - 1],
            share_send_sem.at[step - 1],
            share_recv_sem.at[step - 1],
            beside(target * 2 + parity),
        )

    for step in range(1, chips + 1):
        block = lax.rem(chip + step, chips)

        @pl.loop(1, reach)
        def _(place):
            near_return(place, block).wait_recv()

        if step < chips:
            share_send[step - 1] = routed_sum(0, near_count, near_back[block]).astype(BF16)
            share_copy(step).start()
        else:
            sums[...] = mixer[chip].astype(F32) + routed_sum(0, near_count, near_back[chip])

    @pl.loop(0, groups)
    def _(group):
        for place in range(span):
            give_back(group * span + place).wait_recv()
        sums[...] += routed_sum(near_count + group * rows, rows, far_back[group])

    for step in range(1, chips):
        share_copy(step).wait_recv()
        sums[...] += share_recv[step - 1].astype(F32)

    for step in range(1, chips):
        share_copy(step).wait_send()

    @pl.loop(0, reach)
    def _(place):
        give_back(place).wait_send()

    for source in range(chips):
        @pl.loop(1, reach)
        def _(place):
            near_return(place, source).wait_send()


def local(
    residual,
    queries,
    key_rows,
    value_rows,
    diff_scale,
    head_gain,
    out_weight,
    norm_gain,
    gate_weight,
    up_weight,
    down_weight,
    expert_ids,
    route_logit,
):
    sp_size = lax.axis_size("sp")
    tp_size = lax.axis_size("tp")
    tokens, heads, width = value_rows.shape
    feats = residual.shape[1]
    tops = expert_ids.shape[1]
    cap = -(-(2 * tokens * tops // sp_size) // 16) * 16
    reach = sp_size // 2
    groups = math.gcd(reach, 2)
    rows = reach // groups * cap
    near_count = reach * cap
    units = gate_weight.shape[2]
    chips = tp_size // 2
    peers = max(chips - 1, 1)
    chunk = 2 * units // 16
    ext = units // 4 if units % 1024 == 0 else 0
    kept_ext = max(ext, 128)
    pieces = 2 * ((units - ext) // chunk)
    dma = pltpu.SemaphoreType.DMA
    vmem = pl.BlockSpec(memory_space=pltpu.VMEM)
    hbm = pl.BlockSpec(memory_space=pl.ANY)
    return pl.pallas_call(
        functools.partial(layer_kernel, sp_size, tp_size, groups, cap, ext, chunk),
        out_shape=jax.ShapeDtypeStruct((tokens, feats), F32),
        in_specs=[
            hbm,
            hbm,
            hbm,
            hbm,
            pl.BlockSpec(memory_space=pltpu.SMEM),
            vmem,
            hbm,
            vmem,
            hbm,
            hbm,
            hbm,
            vmem,
            vmem,
        ],
        out_specs=vmem,
        scratch_shapes=[
            pltpu.VMEM((tokens, feats), BF16),
            pltpu.VMEM((3, tokens, heads, width), BF16),
            pltpu.VMEM((2, heads, tokens, width), BF16),
            pltpu.VMEM((sp_size, heads, 2, tokens, width), BF16),
            pltpu.VMEM((heads * 2, 1, tokens), F32),
            pltpu.VMEM((heads * 2, width + 16, tokens), F32),
            pltpu.VMEM((heads, tp_size, tokens, width), BF16),
            pltpu.VMEM(out_weight.shape, BF16),
            pltpu.VMEM((chips, tokens, feats), BF16),
            pltpu.VMEM((tops, tokens), jnp.int32),
            pltpu.VMEM((reach, chips, cap, feats), BF16),
            pltpu.VMEM((reach, cap, feats), BF16),
            pltpu.VMEM((tp_size, near_count, feats), BF16),
            pltpu.VMEM((groups, tp_size, rows, feats), BF16),
            pltpu.VMEM((near_count, tp_size * feats), BF16),
            pltpu.VMEM((2, near_count, units), BF16),
            pltpu.VMEM((groups, 2, rows, units), BF16),
            pltpu.VMEM((groups, chips, 2, rows, kept_ext), BF16),
            pltpu.VMEM((chips, 2, near_count, kept_ext), BF16),
            pltpu.VMEM((chips, 2 * units, feats), BF16),
            pltpu.VMEM((peers, 2 * kept_ext, feats), BF16),
            pltpu.VMEM((tokens, feats), F32),
            pltpu.VMEM((groups, rows, feats), F32),
            pltpu.VMEM((groups, peers, rows, feats), BF16),
            pltpu.VMEM((groups, peers, rows, feats), BF16),
            pltpu.VMEM((chips, near_count, feats), BF16),
            pltpu.VMEM((groups, rows, feats), BF16),
            pltpu.VMEM((chips, near_count, feats), BF16),
            pltpu.VMEM((groups, rows, feats), BF16),
            pltpu.VMEM((peers, tokens, feats), BF16),
            pltpu.VMEM((peers, tokens, feats), BF16),
            pltpu.VMEM(gate_weight.shape[1:], BF16),
            pltpu.VMEM(up_weight.shape[1:], BF16),
            dma((5 + 2 * peers,)),
            dma((3,)),
            dma((sp_size,)),
            dma((sp_size,)),
            dma((sp_size,)),
            dma(()),
            dma(()),
            dma((peers, pieces)),
            dma((chips, pieces)),
            dma((heads, tp_size)),
            dma((heads, tp_size)),
            dma((peers,)),
            dma((chips,)),
            dma((reach, chips)),
            dma((reach, chips)),
            dma((reach,)),
            dma((reach,)),
            dma((chips,)),
            dma((chips,)),
            dma((groups, reach // groups, tp_size)),
            dma((groups, reach // groups, tp_size)),
            dma((groups + 1,)),
            dma((groups + 1,)),
            dma((groups + 1, peers)),
            dma((groups + 1, chips, 2)),
            dma((groups + 1, peers)),
            dma((groups, peers)),
            dma((groups, peers)),
            dma((reach, chips)),
            dma((reach, chips)),
            dma((reach,)),
            dma((reach,)),
            dma((peers,)),
            dma((peers,)),
        ],
        compiler_params=pltpu.CompilerParams(
            collective_id=0, has_side_effects=True, vmem_limit_bytes=56 * 1024 * 1024
        ),
    )(
        residual,
        queries,
        key_rows,
        value_rows,
        diff_scale,
        head_gain[None],
        out_weight,
        norm_gain[None],
        gate_weight[0],
        up_weight[0],
        down_weight[0],
        expert_ids.T,
        route_logit.T,
    ).astype(BF16)


def solution(mesh):
    return jax.shard_map(
        local,
        mesh=mesh,
        in_specs=(
            P("sp", "tp"),
            P("sp", "tp", None),
            P("sp", "tp", None),
            P("sp", "tp", None),
            P("tp"),
            P(),
            P(None, "tp"),
            P(),
            P("sp", None, "tp"),
            P("sp", None, "tp"),
            P("sp", None, "tp"),
            P("sp", None),
            P("sp", None),
        ),
        out_specs=P("sp", "tp"),
        check_vma=False,
    )
```
